32 devices in a mesh: rep: 2 (over x), fs: 8 (over z, y), tp: 2 (over core).
Axes of the slice: x: 2, y: 2, z: 4, core: 2. Of those that a mesh axis runs over, the one named last changes fastest.
Arguments:
- tokens: bfloat16 [8192, 2048], P(('rep', 'fs')), may hold values from -6 to 6
- mixer_gain: float32 [2048], replicated, may hold values from 0.1 to 1.9
- pool_input: float32 [2048, 1024], P('fs', 'tp'), may hold values from -0.125 to 0.125
- input_scale: float32 [1024], P('tp'), may hold values from 0.5 to 2
- group_mix: float32 [128, 1024], P(None, 'tp'), may hold values from -0.5 to 0.5
- group_scale: float32 [1024], P('tp'), may hold values from 0.5 to 2
- pool_output: float32 [2048, 1024], P('fs', 'tp'), may hold values from -0.1875 to 0.1875
- output_scale: float32 [2048], P('fs'), may hold values from 0.5 to 2
- channel_gain: float32 [2048], replicated, may hold values from 0.1 to 1.9
- gate_weight: float32 [2048, 5632], P('fs', 'tp'), may hold values from -0.125 to 0.125
- gate_scale: float32 [5632], P('tp'), may hold values from 0.5 to 2
- up_weight: float32 [2048, 5632], P('fs', 'tp'), may hold values from -0.125 to 0.125
- up_scale: float32 [5632], P('tp'), may hold values from 0.5 to 2
- down_weight: float32 [2048, 5632], P('fs', 'tp'), may hold values from -0.078125 to 0.078125
- down_scale: float32 [2048], P('fs'), may hold values from 0.5 to 2
Outputs:
- layer_out: bfloat16 [8192, 2048], P(('rep', 'fs'))
The draws below stay inside these ranges and needn't reach their ends.
All inputs are finite; a program needn't handle non-finite values.
Results may differ from the reference program's by a relative error of at most 0.02.
Values may be sent and summed in bfloat16 or wider, within the bound.
No kernel may reach another device: no remote copies, remote signals or barrier semaphores. Data moves between devices by JAX's collectives and lax.ppermute only.
A program may use at most 128 MiB of HBM per device.

```python
import math
import jax
import jax.numpy as jnp
from jax import lax

D = 2048
FF = 5632
POOL_GROUP = 256
MAP_WIDTH = 128
POOL_WIDTH = 1024
SEQ = 512
TOKENS = 8192
N_TP = 2


def block_levels(stream_key, shape, cuts, smallest, high):
    gain = 1.0
    for dim, parts in cuts:
        draws = jax.random.uniform(jax.random.fold_in(jax.random.fold_in(stream_key, 6), dim), (parts,), jnp.float32, smallest / len(cuts), high / len(cuts))
        gain = gain * jnp.repeat(jnp.exp(draws), shape[dim] // parts).reshape((-1,) + (1,) * (len(shape) - 1 - dim))
    return gain


def normal_values(stream_key, extent, width, bound, shards=(), kind=jnp.bfloat16):
    entries = width * jax.random.normal(stream_key, extent, jnp.float32)
    if shards:
        entries = entries * block_levels(stream_key, extent, shards, -0.22, 0.18)
    return jnp.clip(entries, -bound, bound).astype(kind)


def setup_inputs(seed: int = 0) -> dict:
    key_list = jax.random.split(jax.random.key(seed), 16)
    return {
        "tokens": normal_values(key_list[0], (TOKENS, D), 1.0, 6.0, ((0, 16),)),
        "mixer_gain": jnp.clip(1.0 + 0.18 * jax.random.normal(key_list[1], (D,), jnp.float32), 0.1, 1.9),
        "pool_input": normal_values(key_list[2], (D, POOL_WIDTH), D ** -0.5, 0.125, ((0, 8), (1, 2)), jnp.float32),
        "input_scale": jnp.clip(jnp.exp(math.log(2.0) - 1.3862944 * jax.random.uniform(key_list[3], (POOL_WIDTH,), jnp.float32) ** block_levels(key_list[3], (POOL_WIDTH,), ((0, 2),), -0.2, 0.2)), 0.5, 2.0),
        "group_mix": normal_values(key_list[4], (MAP_WIDTH, POOL_WIDTH), MAP_WIDTH ** -0.5, 0.5, ((1, 2),), jnp.float32),
        "group_scale": jnp.clip(jnp.exp(math.log(2.0) - 1.3862944 * jax.random.uniform(key_list[5], (POOL_WIDTH,), jnp.float32) ** block_levels(key_list[5], (POOL_WIDTH,), ((0, 2),), -0.2, 0.2)), 0.5, 2.0),
        "pool_output": normal_values(key_list[6], (D, POOL_WIDTH), POOL_WIDTH ** -0.5, 0.1875, ((0, 8), (1, 2)), jnp.float32),
        "output_scale": jnp.clip(jnp.exp(math.log(2.0) - 1.3862944 * jax.random.uniform(key_list[7], (D,), jnp.float32) ** block_levels(key_list[7], (D,), ((0, 8),), -0.2, 0.2)), 0.5, 2.0),
        "channel_gain": jnp.clip(1.0 + 0.18 * jax.random.normal(key_list[8], (D,), jnp.float32), 0.1, 1.9),
        "gate_weight": normal_values(key_list[9], (D, FF), D ** -0.5, 0.125, ((0, 8), (1, 2)), jnp.float32),
        "gate_scale": jnp.clip(jnp.exp(math.log(2.0) - 1.3862944 * jax.random.uniform(key_list[10], (FF,), jnp.float32) ** block_levels(key_list[10], (FF,), ((0, 2),), -0.2, 0.2)), 0.5, 2.0),
        "up_weight": normal_values(key_list[11], (D, FF), D ** -0.5, 0.125, ((0, 8), (1, 2)), jnp.float32),
        "up_scale": jnp.clip(jnp.exp(math.log(2.0) - 1.3862944 * jax.random.uniform(key_list[12], (FF,), jnp.float32) ** block_levels(key_list[12], (FF,), ((0, 2),), -0.2, 0.2)), 0.5, 2.0),
        "down_weight": normal_values(key_list[13], (D, FF), FF ** -0.5, 0.078125, ((0, 8), (1, 2)), jnp.float32),
        "down_scale": jnp.clip(jnp.exp(math.log(2.0) - 1.3862944 * jax.random.uniform(key_list[14], (D,), jnp.float32) ** block_levels(key_list[14], (D,), ((0, 8),), -0.2, 0.2)), 0.5, 2.0),
    }


epsilon = 1e-06

def rms_norm(row_block, gain_row):
    floats = row_block.astype(jnp.float32)
    scaled = floats * lax.rsqrt(lax.optimization_barrier(jnp.mean(floats * floats, axis=-1, keepdims=True)) + epsilon)
    return (scaled * gain_row).astype(jnp.bfloat16)

def block_sum(left_rows, weight_rows, feature_scale, blocks):
    length = left_rows.shape[0]
    block_width = left_rows.shape[1] // blocks
    left_split = left_rows.astype(jnp.float32).reshape(length, blocks, block_width)
    right_split = weight_rows.astype(jnp.bfloat16).astype(jnp.float32).reshape(weight_rows.shape[0], blocks, block_width)
    partials = jnp.einsum('sjc,djc->jsd', left_split, right_split)
    rounded = (partials * feature_scale).astype(jnp.bfloat16)
    rounded = lax.optimization_barrier(rounded)
    return lax.optimization_barrier(jnp.sum(rounded.astype(jnp.float32), axis=0))

def one_layer(row_block, mixer_gain, pool_input, input_scale, group_mix, group_scale, pool_output, output_scale, channel_gain, gate_weight, gate_scale, up_weight, up_scale, down_weight, down_scale):
    length = row_block.shape[0]
    normed = rms_norm(row_block, mixer_gain)
    pool_in = (jnp.dot(normed, pool_input.astype(jnp.bfloat16), preferred_element_type=jnp.float32) * input_scale).astype(jnp.bfloat16)
    grouped_in = pool_in.astype(jnp.float32).reshape(length, 4, POOL_GROUP)
    running = jnp.concatenate([jnp.zeros((1, 4, POOL_GROUP), jnp.float32), jnp.cumsum(grouped_in, axis=0)], axis=0)
    places = jnp.arange(length, dtype=jnp.int32)
    window_means = []
    for group_index in range(4):
        window = 2 ** (group_index + 1)
        first_row = jnp.maximum(places + 1 - window, 0).astype(jnp.int32)
        counts = (places + 1 - first_row).astype(jnp.float32)
        window_sum = running[1:, group_index] - running[first_row, group_index]
        window_means.append(window_sum / counts[:, None] - grouped_in[:, group_index])
    pooled = jnp.stack(window_means, axis=1).astype(jnp.bfloat16).reshape(length, POOL_WIDTH)
    map_blocks = POOL_WIDTH // MAP_WIDTH
    mix_matrix = group_mix.astype(jnp.bfloat16).astype(jnp.float32).reshape(MAP_WIDTH, map_blocks, MAP_WIDTH)
    mixed_raw = jnp.einsum('sgc,cgd->sgd', pooled.astype(jnp.float32).reshape(length, map_blocks, MAP_WIDTH), mix_matrix).reshape(length, POOL_WIDTH)
    grouped = (mixed_raw * group_scale).astype(jnp.bfloat16)
    mixer_out = block_sum(grouped, pool_output, output_scale, N_TP)
    middle = (row_block.astype(jnp.float32) + mixer_out).astype(jnp.bfloat16)
    second = rms_norm(middle, channel_gain)
    gate_sum = jnp.dot(second, gate_weight.astype(jnp.bfloat16), preferred_element_type=jnp.float32) * gate_scale
    up_sum = jnp.dot(second, up_weight.astype(jnp.bfloat16), preferred_element_type=jnp.float32) * up_scale
    hidden = (jax.nn.silu(gate_sum) * up_sum).astype(jnp.bfloat16)
    channel_out = block_sum(hidden, down_weight, down_scale, N_TP)
    return (middle.astype(jnp.float32) + channel_out).astype(jnp.bfloat16)

def reference(tokens, mixer_gain, pool_input, input_scale, group_mix, group_scale, pool_output, output_scale, channel_gain, gate_weight, gate_scale, up_weight, up_scale, down_weight, down_scale):
    sequences = tokens.reshape(TOKENS // SEQ, SEQ, D)

    def each_sequence(row_block):
        return one_layer(row_block, mixer_gain, pool_input, input_scale, group_mix, group_scale, pool_output, output_scale, channel_gain, gate_weight, gate_scale, up_weight, up_scale, down_weight, down_scale)
    results = lax.map(each_sequence, sequences)
    return results.reshape(TOKENS, D)
```

```python
import functools
import jax
import jax.numpy as jnp
from jax import lax
from jax.experimental import pallas as pl
from jax.experimental.pallas import tpu as pltpu
from jax.sharding import PartitionSpec as P

POOL_GROUP = 256
BF = jnp.bfloat16
F32 = jnp.float32
epsilon = 1e-06


def rms_norm(row_block, gain_row):
    floats = row_block.astype(F32)
    scaled = floats * lax.rsqrt(jnp.mean(floats * floats, axis=-1, keepdims=True) + epsilon)
    return (scaled * gain_row).astype(BF)


def transposed_product(left_rows, weight_rows):
    return lax.dot_general(
        left_rows, weight_rows, (((1,), (1,)), ((), ())), preferred_element_type=F32
    )


def plain_body(
    tokens, mixer_gain, pool_input, input_scale, group_mix, group_scale, pool_output, output_scale,
    channel_gain, gate_weight, gate_scale, up_weight, up_scale, down_weight, down_scale,
):
    def gather(value):
        return lax.all_gather(value, "fs", axis=0, tiled=True)

    length = tokens.shape[0]
    block_width, local_width = group_mix.shape
    normed = rms_norm(tokens, mixer_gain)
    input_full = gather(pool_input.astype(BF))
    output_full = gather(pool_output.astype(BF))
    output_feature, down_feature = gather(output_scale), gather(down_scale)
    pool_in = (jnp.dot(normed, input_full, preferred_element_type=F32) * input_scale).astype(BF)
    places = jnp.arange(length, dtype=jnp.int32)
    offsets = places[:, None] - places[None, :]
    chunk = min(POOL_GROUP, local_width)
    pieces = []
    for piece in range(local_width // chunk):
        group_index = (lax.axis_index("tp") * local_width + piece * chunk) // POOL_GROUP
        window = lax.shift_left(jnp.int32(2), group_index.astype(jnp.int32))
        band_mask = ((offsets >= 0) & (offsets < window)).astype(BF)
        columns = pool_in[:, piece * chunk : (piece + 1) * chunk]
        window_sums = jnp.dot(band_mask, columns, preferred_element_type=F32)
        counts = jnp.minimum(places + 1, window).astype(F32)
        pieces.append((window_sums / counts[:, None] - columns.astype(F32)).astype(BF))
    pooled = jnp.concatenate(pieces, axis=1)
    local_blocks = local_width // block_width
    mixed_raw = jnp.einsum(
        "sgc,cgd->sgd",
        pooled.reshape(length, local_blocks, block_width),
        group_mix.astype(BF).reshape(block_width, local_blocks, block_width),
        preferred_element_type=F32,
    ).reshape(length, local_width)
    grouped = (mixed_raw * group_scale).astype(BF)
    partial_value = (transposed_product(grouped, output_full) * output_feature).astype(BF)
    mixer_out = lax.psum(partial_value, "tp").astype(F32)
    middle = (tokens.astype(F32) + mixer_out).astype(BF)
    second = rms_norm(middle, channel_gain)
    gate_sum = jnp.dot(second, gather(gate_weight.astype(BF)), preferred_element_type=F32)
    up_sum = jnp.dot(second, gather(up_weight.astype(BF)), preferred_element_type=F32)
    hidden = (jax.nn.silu(gate_sum * gate_scale) * (up_sum * up_scale)).astype(BF)
    projected = transposed_product(hidden, gather(down_weight.astype(BF)))
    channel_part = (projected * down_feature).astype(BF)
    channel_out = lax.psum(channel_part, "tp").astype(F32)
    return (middle.astype(F32) + channel_out).astype(BF)


def mixer_kernel(n_ring, half, *refs):
    place, tokens, gain, in_scale, mix, mix_scale, out_scale = refs[:7]
    own, other = refs[7:9]
    rest = refs[9 : 9 + 4 * (n_ring - 1)]
    part, weights, sems = refs[9 + 4 * (n_ring - 1) :]
    rep, col, core = place[0], place[1], place[2]
    copies = []

    def bring(source, ring, y, h, rows):
        start = pl.multiple_of(ring * 4 * half + y * 2 * half + h * half, half)
        copy = pltpu.make_async_copy(
            source, weights.at[:, pl.ds(start, rows), :], sems.at[len(copies)]
        )
        copy.start()
        copies.append(copy)

    bring(own, 0, col, 0, 2 * half)
    bring(other, 0, 1 - col, 0, 2 * half)
    for k in range(1, n_ring):
        mine, across, beside, corner = rest[4 * (k - 1) : 4 * k]
        bring(mine, k, col, rep, half)
        bring(across, k, col, 1 - rep, half)
        bring(beside, k, 1 - col, rep, half)
        bring(corner, k, 1 - col, 1 - rep, half)
    floats = tokens[...].astype(F32)
    scaled = floats * lax.rsqrt(jnp.mean(floats * floats, axis=-1, keepdims=True) + epsilon)
    normed = (scaled * gain[...]).astype(BF)
    for copy in copies:
        copy.wait()
    pool_in = jnp.dot(normed, weights[0], preferred_element_type=F32)
    pool_in = (pool_in * in_scale[...]).astype(BF)
    length, width = pool_in.shape
    offsets = lax.broadcasted_iota(jnp.int32, (length, length), 0) - lax.broadcasted_iota(
        jnp.int32, (length, length), 1
    )
    places = lax.broadcasted_iota(jnp.int32, (length, 1), 0)
    block = mix.shape[0]
    grouped = []
    for piece in range(width // POOL_GROUP):
        window = lax.shift_left(jnp.int32(2), core * (width // POOL_GROUP) + piece)
        band = jnp.where((offsets >= 0) & (offsets < window), 1.0, 0.0).astype(BF)
        columns = pool_in[:, piece * POOL_GROUP : (piece + 1) * POOL_GROUP]
        sums = jnp.dot(band, columns, preferred_element_type=F32)
        counts = jnp.minimum(places + 1, window).astype(F32)
        pooled = (sums / counts - columns.astype(F32)).astype(BF)
        for b in range(POOL_GROUP // block):
            lo = piece * POOL_GROUP + b * block
            mixed = jnp.dot(
                pooled[:, b * block : (b + 1) * block],
                mix[:, lo : lo + block].astype(BF),
                preferred_element_type=F32,
            )
            grouped.append((mixed * mix_scale[:, lo : lo + block]).astype(BF))
    grouped = jnp.concatenate(grouped, axis=1)
    part[...] = (transposed_product(grouped, weights[1]) * out_scale[...]).astype(BF)


def run_mixer(place, tokens, gain, in_scale, mix, mix_scale, out_scale, own, other, rest):
    length, width = tokens.shape
    half = own.shape[1] // 2
    n_ring = 1 + len(rest) // 4
    vmem = pl.BlockSpec(memory_space=pltpu.VMEM)
    hbm = pl.BlockSpec(memory_space=pl.ANY)
    n_copies = 2 + len(rest)
    return pl.pallas_call(
        functools.partial(mixer_kernel, n_ring, half),
        out_shape=jax.ShapeDtypeStruct((length, width), BF),
        in_specs=[pl.BlockSpec(memory_space=pltpu.SMEM)] + [vmem] * 6 + [hbm] * n_copies,
        out_specs=vmem,
        scratch_shapes=[
            pltpu.VMEM((2, width, own.shape[2]), BF),
            pltpu.SemaphoreType.DMA((n_copies,)),
        ],
        name="mixer",
        cost_estimate=pl.CostEstimate(flops=5_000_000_000, bytes_accessed=10_000_000, transcendentals=512),
    )(place, tokens, gain, in_scale, mix, mix_scale, out_scale, own, other, *rest)


def gated_kernel(n_blocks, n_weights, keep, *refs):
    scale = refs[0]
    rows = refs[1 : 1 + n_blocks]
    parts = refs[1 + n_blocks : 1 + n_blocks + n_weights]
    mine, others, weights, stage, row_sems, sems = refs[1 + n_blocks + n_weights :]
    shard = parts[0].shape[0]
    aligned = keep // 128 * 128
    length = rows[0].shape[0]

    def row_copy(i):
        return pltpu.make_async_copy(rows[i], stage.at[i % 2], row_sems.at[i % 2])

    copies = [
        pltpu.make_async_copy(p, weights.at[pl.ds(i * shard, shard), :], sems.at[i])
        for i, p in enumerate(parts)
    ]
    row_copy(0).start()
    for copy in copies:
        copy.start()
    row_copy(0).wait()
    for copy in copies:
        copy.wait()
    for i in range(n_blocks):
        if i + 1 < n_blocks:
            row_copy(i + 1).start()
        sums = jnp.dot(stage[i % 2], weights[...], preferred_element_type=F32) * scale[...]
        out = mine if i < n_blocks // 2 else others
        at = pl.ds((i % (n_blocks // 2)) * length, length)
        if aligned:
            gate, up = sums[:, :aligned], sums[:, aligned : 2 * aligned]
            out[at, :aligned] = (jax.nn.silu(gate) * up).astype(BF)
        if keep > aligned:
            tail = keep - aligned
            gate, up = sums[:, 2 * aligned : 2 * aligned + tail], sums[:, 2 * aligned + tail :]
            out[at, aligned:keep] = (jax.nn.silu(gate) * up).astype(BF)
        if i + 1 < n_blocks:
            row_copy(i + 1).wait()


def run_gated(scale, rows, parts):
    length, width = rows[0].shape
    both = parts[0].shape[1]
    keep = both // 2
    vmem = pl.BlockSpec(memory_space=pltpu.VMEM)
    hbm = pl.BlockSpec(memory_space=pl.ANY)
    half_shape = jax.ShapeDtypeStruct((length * len(rows) // 2, keep), BF)
    return pl.pallas_call(
        functools.partial(gated_kernel, len(rows), len(parts), keep),
        out_shape=(half_shape, half_shape),
        in_specs=[vmem] + [hbm] * (len(rows) + len(parts)),
        out_specs=(vmem, vmem),
        scratch_shapes=[
            pltpu.VMEM((width, both), BF),
            pltpu.VMEM((2, length, width), BF),
            pltpu.SemaphoreType.DMA((2,)),
            pltpu.SemaphoreType.DMA((len(parts),)),
        ],
        name="gated",
        cost_estimate=pl.CostEstimate(flops=12_000_000_000, bytes_accessed=20_000_000, transcendentals=1_500_000),
    )(scale, *rows, *parts)


def down_kernel(hidden, first, second, scale, out):
    width = first.shape[1]
    for j, weight in enumerate((first, second)):
        sums = jnp.dot(hidden[...], weight[...], preferred_element_type=F32)
        out[:, j * width : (j + 1) * width] = (sums * scale[:, j * width : (j + 1) * width]).astype(BF)


def run_down(hidden, first, second, scale):
    rows, keep = hidden.shape
    width = first.shape[1]
    block = min(rows, 256)
    whole = lambda shape: pl.BlockSpec(shape, lambda i: (0, 0))
    return pl.pallas_call(
        down_kernel,
        grid=(rows // block,),
        out_shape=jax.ShapeDtypeStruct((rows, 2 * width), BF),
        in_specs=[
            pl.BlockSpec((block, keep), lambda i: (i, 0)),
            whole((keep, width)),
            whole((keep, width)),
            whole((1, 2 * width)),
        ],
        out_specs=pl.BlockSpec((block, 2 * width), lambda i: (i, 0)),
        name="down",
        cost_estimate=pl.CostEstimate(flops=750_000_000, bytes_accessed=3_000_000, transcendentals=0),
    )(hidden, first, second, scale)


def shared_body(
    n_fs,
    tokens, mixer_gain, pool_input, input_scale, group_mix, group_scale, pool_output, output_scale,
    channel_gain, gate_weight, gate_scale, up_weight, up_scale, down_weight, down_scale,
):
    n_ring = n_fs // 2
    rep, fs, core = lax.axis_index("rep"), lax.axis_index("fs"), lax.axis_index("tp")
    ring, col = fs // 2, fs % 2
    length, width = tokens.shape
    shard = pool_input.shape[0]
    half = shard // 2
    block = width // n_ring
    rows = length // 2
    quarter = gate_weight.shape[1] // 4

    swap = [(0, 1), (1, 0)]
    col_swap = [(i, i ^ 1) for i in range(n_fs)]
    diagonal = [
        (a * n_fs + i, (1 - a) * n_fs + (i ^ 1)) for a in range(2) for i in range(n_fs)
    ]

    def across(value):
        return lax.ppermute(value, "rep", swap)

    def beside(value):
        return lax.ppermute(value, "fs", col_swap)

    def corner(value):
        return lax.ppermute(value, ("rep", "fs"), diagonal)

    def partner(value):
        return lax.ppermute(value, "tp", swap)

    def around(value, steps):
        return lax.ppermute(
            value, "fs", [(i, (i + 2 * steps) % n_fs) for i in range(n_fs)]
        )

    def place_of(k):
        return ((ring - k) % n_ring) * block

    def turned(value):
        return jnp.concatenate(
            [lax.dynamic_slice_in_dim(value, place_of(k), block, axis=-1) for k in range(n_ring)],
            axis=-1,
        )

    own = jnp.stack([pool_input.astype(BF), pool_output.astype(BF)])
    mine = [lax.dynamic_slice_in_dim(own, rep * half, half, axis=1)]
    mine += [around(mine[0], k) for k in range(1, n_ring)]
    other = beside(own)
    rest = []
    for k in range(1, n_ring):
        next_to = beside(mine[k])
        rest += [mine[k], across(mine[k]), next_to, across(next_to)]

    own_scale = jnp.stack([output_scale, down_scale])
    other_scale = beside(own_scale)
    pair = jnp.where(
        col == 0,
        jnp.stack([own_scale, other_scale], axis=1),
        jnp.stack([other_scale, own_scale], axis=1),
    )
    pairs = [pair] + [around(pair, k) for k in range(1, n_ring)]
    out_scale = jnp.concatenate([p[0].reshape(1, block) for p in pairs], axis=1)
    down_scales = [p[1].reshape(1, block) for p in pairs]

    gate_half = lax.dynamic_slice_in_dim(gate_weight, rep * 2 * quarter, 2 * quarter, axis=1).astype(BF)
    up_half = lax.dynamic_slice_in_dim(up_weight, rep * 2 * quarter, 2 * quarter, axis=1).astype(BF)
    down_half = lax.dynamic_slice_in_dim(down_weight, rep * 2 * quarter, 2 * quarter, axis=1).astype(BF).T
    aligned = quarter // 128 * 128

    def packed(gate, up):
        cut = [gate[:, :aligned], up[:, :aligned], gate[:, aligned:], up[:, aligned:]]
        return jnp.concatenate(cut, axis=1)

    def streams(low, high):
        kept = jnp.where(col == 0, low, high)
        received = beside(jnp.where(col == 0, high, low))
        starts = (jnp.where(col == 0, kept, received), jnp.where(col == 0, received, kept))
        chains = []
        for start in starts:
            chain = [start]
            for _ in range(1, n_ring):
                chain.append(around(chain[-1], 1))
            chains.append(chain)
        return chains

    gated_chains = streams(
        packed(gate_half[:, :quarter], up_half[:, :quarter]),
        packed(gate_half[:, quarter:], up_half[:, quarter:]),
    )
    down_chains = streams(down_half[:quarter], down_half[quarter:])
    at = (rep * 2 + col) * quarter
    gated_scale = packed(
        lax.dynamic_slice_in_dim(gate_scale, at, quarter)[None],
        lax.dynamic_slice_in_dim(up_scale, at, quarter)[None],
    )

    place = jnp.stack([rep, col, core]).astype(jnp.int32)
    tokens = turned(tokens)
    part = run_mixer(
        place, tokens, turned(mixer_gain)[None], input_scale[None], group_mix, group_scale[None],
        out_scale, own, other, rest,
    )
    mixer_out = part.astype(F32) + partner(part).astype(F32)
    middle = (tokens.astype(F32) + mixer_out).astype(BF)
    second = rms_norm(middle, turned(channel_gain)[None])

    here = lax.dynamic_slice_in_dim(second, core * rows, rows)
    there = lax.dynamic_slice_in_dim(second, (1 - core) * rows, rows)
    arrived = [across(here), beside(here), corner(here)]
    blocks = [here] + arrived + [there] + [partner(a) for a in arrived]
    weights = [gated_chains[c][k] for k in range(n_ring) for c in range(2)]
    hidden_mine, hidden_others = run_gated(gated_scale, blocks, weights)

    middle_mine = lax.dynamic_slice_in_dim(middle, core * rows, rows)
    result = jnp.zeros((length, width), BF)
    for k in range(n_ring):
        pieces = (down_chains[0][k], down_chains[1][k], down_scales[k])
        away = partner(run_down(hidden_others, *pieces))
        kept = run_down(hidden_mine, *pieces)
        sums = [
            kept[j * rows : (j + 1) * rows].astype(F32) + away[j * rows : (j + 1) * rows].astype(F32)
            for j in range(4)
        ]
        total = middle_mine[:, k * block : (k + 1) * block].astype(F32) + sums[0]
        total += across(sums[1].astype(BF)).astype(F32)
        total += beside(sums[2].astype(BF)).astype(F32)
        total += corner(sums[3].astype(BF)).astype(F32)
        total = total.astype(BF)
        result = lax.dynamic_update_slice(result, total, (core * rows, place_of(k)))
        result = lax.dynamic_update_slice(result, partner(total), ((1 - core) * rows, place_of(k)))
    return result


def solution(mesh):
    in_specs = (
        P(("rep", "fs"), None), P(), P("fs", "tp"), P("tp"), P(None, "tp"), P("tp"), P("fs", "tp"),
        P("fs"), P(), P("fs", "tp"), P("tp"), P("fs", "tp"), P("tp"), P("fs", "tp"), P("fs"),
    )
    out_specs = P(("rep", "fs"), None)
    n_rep, n_fs, n_tp = (mesh.shape[a] for a in ("rep", "fs", "tp"))

    def body(*args):
        shard, pooled = args[2].shape
        hidden = args[9].shape[1]
        fits = n_rep == 2 and n_tp == 2 and n_fs % 2 == 0 and shard % 32 == 0
        fits = fits and pooled % POOL_GROUP == 0 and hidden % 256 == 0
        if fits:
            return shared_body(n_fs, *args)
        return plain_body(*args)

    return jax.shard_map(body, mesh=mesh, in_specs=in_specs, out_specs=out_specs, check_vma=False)
```

```python
import functools
import jax
import jax.numpy as jnp
from jax import lax
from jax.experimental import pallas as pl
from jax.experimental.pallas import tpu as pltpu
from jax.sharding import PartitionSpec as P


POOL_GROUP = 256
BF = jnp.bfloat16
F32 = jnp.float32
epsilon = 1e-06


def rms_norm(row_block, gain_row):
    floats = row_block.astype(F32)
    scaled = floats * lax.rsqrt(jnp.mean(floats * floats, axis=-1, keepdims=True) + epsilon)
    return (scaled * gain_row).astype(BF)


def transposed_product(left_rows, weight_rows):
    return lax.dot_general(
        left_rows, weight_rows, (((1,), (1,)), ((), ())), preferred_element_type=F32
    )


def plain_body(
    tokens, mixer_gain, pool_input, input_scale, group_mix, group_scale, pool_output, output_scale,
    channel_gain, gate_weight, gate_scale, up_weight, up_scale, down_weight, down_scale,
):
    def gather(value):
        return lax.all_gather(value, "fs", axis=0, tiled=True)

    length = tokens.shape[0]
    block_width, local_width = group_mix.shape
    normed = rms_norm(tokens, mixer_gain)
    input_full = gather(pool_input.astype(BF))
    output_full = gather(pool_output.astype(BF))
    output_feature, down_feature = gather(output_scale), gather(down_scale)
    pool_in = (jnp.dot(normed, input_full, preferred_element_type=F32) * input_scale).astype(BF)
    places = jnp.arange(length, dtype=jnp.int32)
    offsets = places[:, None] - places[None, :]
    chunk = min(POOL_GROUP, local_width)
    pieces = []
    for piece in range(local_width // chunk):
        group_index = (lax.axis_index("tp") * local_width + piece * chunk) // POOL_GROUP
        window = lax.shift_left(jnp.int32(2), group_index.astype(jnp.int32))
        band_mask = ((offsets >= 0) & (offsets < window)).astype(BF)
        columns = pool_in[:, piece * chunk : (piece + 1) * chunk]
        window_sums = jnp.dot(band_mask, columns, preferred_element_type=F32)
        counts = jnp.minimum(places + 1, window).astype(F32)
        pieces.append((window_sums / counts[:, None] - columns.astype(F32)).astype(BF))
    pooled = jnp.concatenate(pieces, axis=1)
    local_blocks = local_width // block_width
    mixed_raw = jnp.einsum(
        "sgc,cgd->sgd",
        pooled.reshape(length, local_blocks, block_width),
        group_mix.astype(BF).reshape(block_width, local_blocks, block_width),
        preferred_element_type=F32,
    ).reshape(length, local_width)
    grouped = (mixed_raw * group_scale).astype(BF)
    partial_value = (transposed_product(grouped, output_full) * output_feature).astype(BF)
    mixer_out = lax.psum(partial_value, "tp").astype(F32)
    middle = (tokens.astype(F32) + mixer_out).astype(BF)
    second = rms_norm(middle, channel_gain)
    gate_sum = jnp.dot(second, gather(gate_weight.astype(BF)), preferred_element_type=F32)
    up_sum = jnp.dot(second, gather(up_weight.astype(BF)), preferred_element_type=F32)
    hidden = (jax.nn.silu(gate_sum * gate_scale) * (up_sum * up_scale)).astype(BF)
    projected = transposed_product(hidden, gather(down_weight.astype(BF)))
    channel_part = (projected * down_feature).astype(BF)
    channel_out = lax.psum(channel_part, "tp").astype(F32)
    return (middle.astype(F32) + channel_out).astype(BF)


VMEM = pl.BlockSpec(memory_space=pltpu.VMEM)
SMEM = pl.BlockSpec(memory_space=pltpu.SMEM)
HBM = pl.BlockSpec(memory_space=pltpu.HBM)


def room(mebibytes):
    return pltpu.CompilerParams(vmem_limit_bytes=mebibytes << 20)


def packed_pair(gate, up, keep):
    aligned = keep // 128 * 128
    pieces = [gate[:, :aligned], up[:, :aligned]]
    if keep > aligned:
        gate_tail, up_tail = gate[:, aligned : aligned + 128], up[:, aligned : aligned + 128]
        lane = lax.broadcasted_iota(jnp.int32, gate_tail.shape, 1)
        pieces.append(jnp.where(lane < keep - aligned, gate_tail, pltpu.roll(up_tail, keep - aligned, 1)))
    return pieces


def pack_kernel(place, gate, up, gate_scale, up_scale, kept, sent, scale):
    keep = kept.shape[1] // 2

    def put(out, gates, ups):
        at = 0
        for piece in packed_pair(gates, ups, keep):
            out[:, at : at + piece.shape[1]] = piece.astype(out.dtype)
            at += piece.shape[1]

    low = (gate[...], up[...])
    high = tuple(pltpu.roll(v, keep, 1) for v in low)
    scales = tuple(jnp.broadcast_to(v[...], (8, 2 * keep)) for v in (gate_scale, up_scale))
    high_scales = tuple(pltpu.roll(v, keep, 1) for v in scales)

    @pl.when(place[1] == 0)
    def _():
        put(kept, *low)
        put(sent, *high)
        put(scale, *scales)

    @pl.when(place[1] != 0)
    def _():
        put(kept, *high)
        put(sent, *low)
        put(scale, *high_scales)


def run_pack(place, gate, up, gate_scale, up_scale):
    rows, width = gate.shape
    both = width // 2
    block = min(rows, 64)
    weight = pl.BlockSpec((block, both), lambda i, p: (i, p[0]))
    scale = pl.BlockSpec((1, both), lambda i, p: (0, p[0]))
    out = pl.BlockSpec((block, both), lambda i, p: (i, 0))
    shape = jax.ShapeDtypeStruct((rows, both), BF)
    return pl.pallas_call(
        pack_kernel,
        grid_spec=pltpu.PrefetchScalarGridSpec(
            num_scalar_prefetch=1,
            grid=(rows // block,),
            in_specs=[weight, weight, scale, scale],
            out_specs=(out, out, pl.BlockSpec((8, both), lambda i, p: (0, 0))),
        ),
        out_shape=(shape, shape, jax.ShapeDtypeStruct((8, both), F32)),
        compiler_params=room(12),
        name="pack",
        cost_estimate=pl.CostEstimate(flops=3_000_000_000, bytes_accessed=5_000_000, transcendentals=0),
    )(place, gate, up, gate_scale, up_scale)


def turn_kernel(place, down, kept, sent):
    keep = kept.shape[0]
    low, high = (down[:, i * keep : (i + 1) * keep].T.astype(BF) for i in range(2))

    @pl.when(place[1] == 0)
    def _():
        kept[...] = low
        sent[...] = high

    @pl.when(place[1] != 0)
    def _():
        kept[...] = high
        sent[...] = low


def run_turn(place, down):
    rows, width = down.shape
    block = 128
    out = pl.BlockSpec((width // 4, block), lambda i, p: (0, i))
    shape = jax.ShapeDtypeStruct((width // 4, rows), BF)
    return pl.pallas_call(
        turn_kernel,
        grid_spec=pltpu.PrefetchScalarGridSpec(
            num_scalar_prefetch=1,
            grid=(rows // block,),
            in_specs=[pl.BlockSpec((block, width // 2), lambda i, p: (i, p[0]))],
            out_specs=(out, out),
        ),
        out_shape=(shape, shape),
        compiler_params=room(12),
        name="turn",
        cost_estimate=pl.CostEstimate(flops=2_000_000_000, bytes_accessed=3_000_000, transcendentals=0),
    )(place, down)


def mixer_kernel(n_ring, half, *refs):
    place, normed, in_scale, mix, mix_scale = refs[:5]
    scales = refs[5 : 5 + n_ring]
    own, other = refs[5 + n_ring : 7 + n_ring]
    rest = refs[7 + n_ring : 7 + n_ring + 4 * (n_ring - 1)]
    part_mine, part_away, weights, packed, sems = refs[7 + n_ring + 4 * (n_ring - 1) :]
    rep, col, core = place[0], place[1], place[2]
    copies = []

    def bring(source, ring, y, h, rows):
        start = pl.multiple_of(ring * 4 * half + y * 2 * half + h * half, half)
        copy = pltpu.make_async_copy(
            source, weights.at[:, pl.ds(start, rows), :], sems.at[len(copies)]
        )
        copy.start()
        copies.append(copy)

    bring(own, 0, col, 0, 2 * half)
    bring(other, 0, 1 - col, 0, 2 * half)
    for k in range(1, n_ring):
        mine, across, beside, corner = rest[4 * (k - 1) : 4 * k]
        bring(mine, k, col, rep, half)
        bring(across, k, col, 1 - rep, half)
        bring(beside, k, 1 - col, rep, half)
        bring(corner, k, 1 - col, 1 - rep, half)
    for copy in copies:
        copy.wait()
    pool_in = jnp.dot(normed[...], weights[0], preferred_element_type=F32)
    pool_in = (pool_in * in_scale[...]).astype(BF)
    length, width = pool_in.shape
    offsets = lax.broadcasted_iota(jnp.int32, (length, length), 0) - lax.broadcasted_iota(
        jnp.int32, (length, length), 1
    )
    places = lax.broadcasted_iota(jnp.int32, (length, 1), 0)
    block = mix.shape[0]
    grouped = []
    for piece in range(width // POOL_GROUP):
        window = lax.shift_left(jnp.int32(2), core * (width // POOL_GROUP) + piece)
        band = jnp.where((offsets >= 0) & (offsets < window), 1.0, 0.0).astype(BF)
        columns = pool_in[:, piece * POOL_GROUP : (piece + 1) * POOL_GROUP]
        sums = jnp.dot(band, columns, preferred_element_type=F32)
        counts = jnp.minimum(places + 1, window).astype(F32)
        pooled = (sums / counts - columns.astype(F32)).astype(BF)
        for b in range(POOL_GROUP // block):
            lo = piece * POOL_GROUP + b * block
            mixed = jnp.dot(
                pooled[:, b * block : (b + 1) * block],
                mix[:, lo : lo + block].astype(BF),
                preferred_element_type=F32,
            )
            grouped.append((mixed * mix_scale[:, lo : lo + block]).astype(BF))
    packed[...] = jnp.concatenate(grouped, axis=1)
    rows = length // 2
    for out, h in ((part_away, 1 - core), (part_mine, core)):
        grouped = packed[pl.ds(pl.multiple_of(h * rows, rows), rows), :]
        for k in range(n_ring):
            for j in range(2):
                y = col if j == 0 else 1 - col
                at = pl.ds(pl.multiple_of((2 * k + y) * 2 * half, 2 * half), 2 * half)
                sums = transposed_product(grouped, weights[1, at, :])
                out[:, at] = (sums * scales[k][j, 0:1, :]).astype(BF)


def run_mixer(place, normed, in_scale, mix, mix_scale, scales, own, other, rest):
    length, width = normed.shape
    half = own.shape[1] // 2
    n_ring = len(scales)
    n_copies = 2 + len(rest)
    shape = jax.ShapeDtypeStruct((length // 2, width), BF)
    return pl.pallas_call(
        functools.partial(mixer_kernel, n_ring, half),
        out_shape=(shape, shape),
        in_specs=[SMEM] + [VMEM] * (4 + n_ring) + [HBM] * n_copies,
        out_specs=(VMEM, VMEM),
        scratch_shapes=[
            pltpu.VMEM((2, width, own.shape[2]), BF),
            pltpu.VMEM((length, own.shape[2]), BF),
            pltpu.SemaphoreType.DMA((n_copies,)),
        ],
        compiler_params=room(24),
        name="mixer",
        cost_estimate=pl.CostEstimate(flops=5_000_000_000, bytes_accessed=10_000_000, transcendentals=512),
    )(place, normed, in_scale, mix, mix_scale, *scales, own, other, *rest)


def normed_rows(floats, gain):
    scaled = floats * lax.rsqrt(jnp.mean(floats * floats, axis=-1, keepdims=True) + epsilon)
    return (scaled * gain).astype(BF)


def turn_into(n_ring, ring, source, out):
    block = out.shape[1] // n_ring
    for k in range(n_ring):
        at = lax.rem(ring - k + n_ring, n_ring) * block
        out[:, k * block : (k + 1) * block] = source[:, pl.ds(pl.multiple_of(at, block), block)]


def ready_kernel(n_ring, place, tokens, gain, next_gain, turned, normed, turned_gain, own_gain):
    turn_into(n_ring, place[3], tokens, turned)
    turn_into(n_ring, place[3], gain, own_gain)
    turn_into(n_ring, place[3], next_gain, turned_gain)
    normed[...] = normed_rows(turned[...].astype(F32), own_gain[...])


def run_ready(place, n_ring, tokens, gain, next_gain):
    length, width = tokens.shape
    block = length // 4
    rows = pl.BlockSpec((block, width), lambda i, p: (i, 0))
    line = pl.BlockSpec((1, width), lambda i, p: (0, 0))
    shape = jax.ShapeDtypeStruct((length, width), BF)
    return pl.pallas_call(
        functools.partial(ready_kernel, n_ring),
        grid_spec=pltpu.PrefetchScalarGridSpec(
            num_scalar_prefetch=1,
            grid=(4,),
            in_specs=[rows, line, line],
            out_specs=(rows, rows, line),
            scratch_shapes=[pltpu.VMEM((1, width), F32)],
        ),
        out_shape=(shape, shape, jax.ShapeDtypeStruct((1, width), F32)),
        compiler_params=room(16),
        name="ready",
        cost_estimate=pl.CostEstimate(flops=3_000_000_000, bytes_accessed=6_000_000, transcendentals=512),
    )(place, tokens, gain, next_gain)


def settle_kernel(place, tokens, part, other, gain, middle_mine, here):
    mixer_out = part[...].astype(F32) + other[...].astype(F32)
    middle = (tokens[...].astype(F32) + mixer_out).astype(BF)
    middle_mine[...] = middle
    here[...] = normed_rows(middle.astype(F32), gain[...])


def run_settle(place, tokens, part, other, gain):
    rows, width = part.shape
    block = rows // 4
    shape = jax.ShapeDtypeStruct((rows, width), BF)
    spec = pl.BlockSpec((block, width), lambda i, p: (i, 0))
    return pl.pallas_call(
        settle_kernel,
        grid_spec=pltpu.PrefetchScalarGridSpec(
            num_scalar_prefetch=1,
            grid=(4,),
            in_specs=[
                pl.BlockSpec((block, width), lambda i, p: (p[2] * 4 + i, 0)), spec, spec,
                pl.BlockSpec((1, width), lambda i, p: (0, 0)),
            ],
            out_specs=(spec, spec),
        ),
        out_shape=(shape, shape),
        compiler_params=room(16),
        name="settle",
        cost_estimate=pl.CostEstimate(flops=3_000_000_000, bytes_accessed=9_000_000, transcendentals=512),
    )(place, tokens, part, other, gain)


def gated_kernel(n_rows, starts, n_weights, *refs):
    place, scale, other_scale = refs[:3]
    rows = refs[3 : 3 + n_rows]
    parts = refs[3 + n_rows : 3 + n_rows + n_weights]
    hidden, weights, stage, row_sems, sems = refs[3 + n_rows + n_weights :]
    shard, both = parts[0].shape
    keep = both // 2
    aligned = keep // 128 * 128
    tail = keep - aligned
    copies = []
    for i, p in enumerate(parts):
        y = place[1] if i // 2 % 2 == 0 else 1 - place[1]
        at = pl.ds(pl.multiple_of((i // 4 * 2 + y) * shard, shard), shard)
        lanes = pl.ds(i % 2 * both, both)
        copies.append(pltpu.make_async_copy(p, weights.at[at, lanes], sems.at[i]))
    row_copies = [
        pltpu.make_async_copy(r, stage.at[pl.ds(start, r.shape[0]), :], row_sems.at[i])
        for i, (r, start) in enumerate(zip(rows, starts))
    ]
    for copy in row_copies:
        copy.start()
    for j in range(2):
        for copy in copies[j::2]:
            copy.start()
    for copy in row_copies:
        copy.wait()

    def product(lo, size):
        return jnp.dot(stage[...], weights[:, lo : lo + size], preferred_element_type=F32)

    for j in range(2):
        for copy in copies[j::2]:
            copy.wait()
        line = (scale, other_scale)[j]
        at = 0
        while at < aligned:
            size = min(256, aligned - at)
            gate = product(j * both + at, size) * line[0:1, at : at + size]
            up_at = aligned + at
            up = product(j * both + up_at, size) * line[0:1, up_at : up_at + size]
            hidden[:, j * aligned + at : j * aligned + at + size] = (jax.nn.silu(gate) * up).astype(BF)
            at += size
    if tail:
        first, second = (
            product(j * both + 2 * aligned, 2 * tail) * line[0:1, 2 * aligned :]
            for j, line in enumerate((scale, other_scale))
        )
        lane = lax.broadcasted_iota(jnp.int32, first.shape, 1)
        gate = jnp.where(lane < tail, first, pltpu.roll(second, tail, 1))
        up = jnp.where(lane < tail, pltpu.roll(first, tail, 1), second)
        hidden[:, 2 * aligned :] = (jax.nn.silu(gate) * up).astype(BF)


def run_gated(place, scale, other_scale, rows, parts):
    starts, total = [], 0
    for r in rows:
        starts.append(total)
        total += r.shape[0]
    width = rows[0].shape[1]
    both = parts[0].shape[1]
    return pl.pallas_call(
        functools.partial(gated_kernel, len(rows), tuple(starts), len(parts)),
        out_shape=jax.ShapeDtypeStruct((total, both), BF),
        in_specs=[SMEM, VMEM, VMEM] + [HBM] * (len(rows) + len(parts)),
        out_specs=VMEM,
        scratch_shapes=[
            pltpu.VMEM((width, 2 * both), BF),
            pltpu.VMEM((total, width), BF),
            pltpu.SemaphoreType.DMA((len(rows),)),
            pltpu.SemaphoreType.DMA((len(parts),)),
        ],
        compiler_params=room(34),
        name="gated",
        cost_estimate=pl.CostEstimate(flops=12_000_000_000, bytes_accessed=20_000_000, transcendentals=1_500_000),
    )(place, scale, other_scale, *rows, *parts)


def keep_kernel(k, place, hidden, scale, middle, *refs):
    parts = refs[:4]
    base, outs = refs[4], refs[5:8]
    ends = refs[8]
    keep, width = parts[0].shape
    aligned = keep // 128 * 128
    tail = keep - aligned
    rows = base.shape[0]
    for i in range(2):
        own, other = parts[2 * i : 2 * i + 2]
        y = place[1] if i == 0 else 1 - place[1]
        lanes = pl.ds(pl.multiple_of(y * width, width), width)
        from_lanes = pl.ds(pl.multiple_of((2 * k + y) * width, width), width)
        ends[:tail, :] = own[aligned:, :]
        ends[tail:, :] = other[aligned:, :]
        total = jnp.dot(hidden[:, :aligned], own[:aligned, :], preferred_element_type=F32)
        total += jnp.dot(
            hidden[:, aligned : 2 * aligned], other[:aligned, :], preferred_element_type=F32
        )
        total += jnp.dot(hidden[:, 2 * aligned :], ends[...], preferred_element_type=F32)
        total = total * scale[i, 1:2, :]
        base[:, lanes] = total[:rows, :] + middle[:, from_lanes].astype(F32)
        for j, out in enumerate(outs):
            out[:, lanes] = total[(j + 1) * rows : (j + 2) * rows, :].astype(BF)


def run_keep(place, hidden, scale, middle, parts, k):
    rows = hidden.shape[0] // 4
    keep, width = parts[0].shape
    shape = jax.ShapeDtypeStruct((rows, 2 * width), BF)
    return pl.pallas_call(
        functools.partial(keep_kernel, k),
        in_specs=[SMEM] + [VMEM] * 7,
        out_specs=(VMEM, VMEM, VMEM, VMEM),
        scratch_shapes=[pltpu.VMEM((2 * (keep % 128), width), BF)],
        out_shape=(jax.ShapeDtypeStruct(shape.shape, F32), shape, shape, shape),
        compiler_params=room(20),
        name="keep",
        cost_estimate=pl.CostEstimate(flops=2_000_000_000, bytes_accessed=5_000_000, transcendentals=0),
    )(place, hidden, scale, middle, *parts)


def join_kernel(base, first, second, third, out):
    total = base[...] + first[...].astype(F32) + second[...].astype(F32) + third[...].astype(F32)
    out[...] = total.astype(BF)


def run_join(base, *others):
    return pl.pallas_call(
        join_kernel,
        in_specs=[VMEM] * 4,
        out_specs=VMEM,
        out_shape=jax.ShapeDtypeStruct(base.shape, BF),
        compiler_params=room(8),
        name="join",
        cost_estimate=pl.CostEstimate(flops=1_000_000_000, bytes_accessed=2_000_000, transcendentals=0),
    )(base, *others)


def collect_kernel(n_ring, steps, *refs):
    place = refs[0]
    pieces = refs[1 : 1 + 2 * len(steps)]
    out, sems = refs[-2:]
    rows, width = pieces[0].shape
    copies = []
    for i, piece in enumerate(pieces):
        h = place[2] if i % 2 == 0 else 1 - place[2]
        block = lax.rem(place[3] - steps[i // 2] + n_ring, n_ring)
        at = out.at[
            pl.ds(pl.multiple_of(h * rows, rows), rows),
            pl.ds(pl.multiple_of(block * width, width), width),
        ]
        copy = pltpu.make_async_copy(piece, at, sems.at[i])
        copy.start()
        copies.append(copy)
    for copy in copies:
        copy.wait()


def run_collect(place, n_ring, steps, pieces, into=None):
    rows, width = pieces[0].shape
    extra = [] if into is None else [into]
    return pl.pallas_call(
        functools.partial(collect_kernel, n_ring, steps),
        out_shape=jax.ShapeDtypeStruct((2 * rows, width * n_ring), BF),
        in_specs=[SMEM] + [VMEM] * len(pieces) + [HBM] * len(extra),
        out_specs=HBM,
        input_output_aliases={1 + len(pieces): 0} if extra else {},
        scratch_shapes=[pltpu.SemaphoreType.DMA((len(pieces),))],
        compiler_params=room(12),
        name="collect",
        cost_estimate=pl.CostEstimate(flops=2_000_000_000, bytes_accessed=4_000_000, transcendentals=0),
    )(place, *pieces, *extra)


def shared_body(
    n_fs,
    tokens, mixer_gain, pool_input, input_scale, group_mix, group_scale, pool_output, output_scale,
    channel_gain, gate_weight, gate_scale, up_weight, up_scale, down_weight, down_scale,
):
    n_ring = n_fs // 2
    rep, fs, core = lax.axis_index("rep"), lax.axis_index("fs"), lax.axis_index("tp")
    ring, col = fs // 2, fs % 2
    half = pool_input.shape[0] // 2
    rows = tokens.shape[0] // 2

    swap = [(0, 1), (1, 0)]
    col_swap = [(i, i ^ 1) for i in range(n_fs)]
    diagonal = [
        (a * n_fs + i, (1 - a) * n_fs + (i ^ 1)) for a in range(2) for i in range(n_fs)
    ]

    def across(value):
        return lax.ppermute(value, "rep", swap)

    def beside(value):
        return lax.ppermute(value, "fs", col_swap)

    def corner(value):
        return lax.ppermute(value, ("rep", "fs"), diagonal)

    def partner(value):
        return lax.ppermute(value, "tp", swap)

    def around(value, steps=1):
        return lax.ppermute(
            value, "fs", [(i, (i + 2 * steps) % n_fs) for i in range(n_fs)]
        )

    place = jnp.stack([rep, col, core, ring]).astype(jnp.int32)

    own = jnp.stack([pool_input.astype(BF), pool_output.astype(BF)])
    mine = [lax.dynamic_slice_in_dim(own, rep * half, half, axis=1)]
    mine += [around(mine[0])]
    mine += [around(mine[1], k - 1) for k in range(2, n_ring - 1)]
    mine += [around(mine[0], -1)]
    other = beside(own)
    rest = []
    for k in range(1, n_ring):
        next_to, facing = beside(mine[k]), across(mine[k])
        last = across(next_to)
        rest += [mine[k], facing, next_to, last]

    own_scale = jnp.stack([output_scale, down_scale])
    pair = jnp.stack([own_scale, beside(own_scale)])
    scales = [pair] + [around(pair, k) for k in range(1, n_ring)]

    def streams(kept, sent):
        chains = []
        for start in (kept, beside(sent)):
            chain = [start]
            for _ in range(1, n_ring):
                chain.append(around(chain[-1]))
            chains.append([(c, partner(c)) for c in chain])
        return [chains[0][k] + chains[1][k] for k in range(n_ring)]

    gated_kept, gated_sent, gated_scale = run_pack(place, gate_weight, up_weight, gate_scale[None], up_scale[None])
    gated_parts = streams(gated_kept, gated_sent)
    down_parts = streams(*run_turn(place, down_weight))

    tokens, normed, next_gain = run_ready(place, n_ring, tokens, mixer_gain[None], channel_gain[None])
    part_mine, part_away = run_mixer(
        place, normed, input_scale[None], group_mix, group_scale[None], scales, own,
        other, rest,
    )
    middle_mine, here = run_settle(place, tokens, part_mine, partner(part_away), next_gain)

    ax, ay = across(here), beside(here)
    cut = rows // 2
    far = [across(ay[:cut]), beside(ax[cut:])]
    hidden = run_gated(
        place, gated_scale, partner(gated_scale), [here, ax, ay] + far,
        sum(gated_parts, ()),
    )

    pieces = []
    for k in range(n_ring):
        base, to_x, to_y, to_far = run_keep(place, hidden, scales[k], middle_mine, down_parts[k], k)
        total = run_join(
            base, across(to_x), beside(to_y),
            corner(to_far),
        )
        pieces.append((total, partner(total)))
    early = run_collect(place, n_ring, tuple(range(n_ring - 1)), sum(pieces[:-1], ()))
    return run_collect(place, n_ring, (n_ring - 1,), pieces[-1], early)


def solution(mesh):
    in_specs = (
        P(("rep", "fs"), None), P(), P("fs", "tp"), P("tp"), P(None, "tp"), P("tp"), P("fs", "tp"),
        P("fs"), P(), P("fs", "tp"), P("tp"), P("fs", "tp"), P("tp"), P("fs", "tp"), P("fs"),
    )
    out_specs = P(("rep", "fs"), None)
    n_rep, n_fs, n_tp = (mesh.shape[a] for a in ("rep", "fs", "tp"))
    shared = n_rep == 2 and n_tp == 2 and n_fs == 8

    def body(*args):
        return shared_body(n_fs, *args) if shared else plain_body(*args)

    return jax.shard_map(body, mesh=mesh, in_specs=in_specs, out_specs=out_specs, check_vma=False)
```

```python
import functools
import jax
import jax.numpy as jnp
from jax import lax
from jax.experimental import pallas as pl
from jax.experimental.pallas import tpu as pltpu
from jax.sharding import PartitionSpec as P


POOL_GROUP = 256
BF = jnp.bfloat16
F32 = jnp.float32
epsilon = 1e-06


def rms_norm(row_block, gain_row):
    floats = row_block.astype(F32)
    scaled = floats * lax.rsqrt(jnp.mean(floats * floats, axis=-1, keepdims=True) + epsilon)
    return (scaled * gain_row).astype(BF)


def transposed_product(left_rows, weight_rows):
    return lax.dot_general(
        left_rows, weight_rows, (((1,), (1,)), ((), ())), preferred_element_type=F32
    )


def plain_body(
    tokens, mixer_gain, pool_input, input_scale, group_mix, group_scale, pool_output, output_scale,
    channel_gain, gate_weight, gate_scale, up_weight, up_scale, down_weight, down_scale,
):
    def gather(value):
        return lax.all_gather(value, "fs", axis=0, tiled=True)

    length = tokens.shape[0]
    block_width, local_width = group_mix.shape
    normed = rms_norm(tokens, mixer_gain)
    input_full = gather(pool_input.astype(BF))
    output_full = gather(pool_output.astype(BF))
    output_feature, down_feature = gather(output_scale), gather(down_scale)
    pool_in = (jnp.dot(normed, input_full, preferred_element_type=F32) * input_scale).astype(BF)
    places = jnp.arange(length, dtype=jnp.int32)
    offsets = places[:, None] - places[None, :]
    chunk = min(POOL_GROUP, local_width)
    pieces = []
    for piece in range(local_width // chunk):
        group_index = (lax.axis_index("tp") * local_width + piece * chunk) // POOL_GROUP
        window = lax.shift_left(jnp.int32(2), group_index.astype(jnp.int32))
        band_mask = ((offsets >= 0) & (offsets < window)).astype(BF)
        columns = pool_in[:, piece * chunk : (piece + 1) * chunk]
        window_sums = jnp.dot(band_mask, columns, preferred_element_type=F32)
        counts = jnp.minimum(places + 1, window).astype(F32)
        pieces.append((window_sums / counts[:, None] - columns.astype(F32)).astype(BF))
    pooled = jnp.concatenate(pieces, axis=1)
    local_blocks = local_width // block_width
    mixed_raw = jnp.einsum(
        "sgc,cgd->sgd",
        pooled.reshape(length, local_blocks, block_width),
        group_mix.astype(BF).reshape(block_width, local_blocks, block_width),
        preferred_element_type=F32,
    ).reshape(length, local_width)
    grouped = (mixed_raw * group_scale).astype(BF)
    partial_value = (transposed_product(grouped, output_full) * output_feature).astype(BF)
    mixer_out = lax.psum(partial_value, "tp").astype(F32)
    middle = (tokens.astype(F32) + mixer_out).astype(BF)
    second = rms_norm(middle, channel_gain)
    gate_sum = jnp.dot(second, gather(gate_weight.astype(BF)), preferred_element_type=F32)
    up_sum = jnp.dot(second, gather(up_weight.astype(BF)), preferred_element_type=F32)
    hidden = (jax.nn.silu(gate_sum * gate_scale) * (up_sum * up_scale)).astype(BF)
    projected = transposed_product(hidden, gather(down_weight.astype(BF)))
    channel_part = (projected * down_feature).astype(BF)
    channel_out = lax.psum(channel_part, "tp").astype(F32)
    return (middle.astype(F32) + channel_out).astype(BF)


VMEM = pl.BlockSpec(memory_space=pltpu.VMEM)
SMEM = pl.BlockSpec(memory_space=pltpu.SMEM)
HBM = pl.BlockSpec(memory_space=pltpu.HBM)


def room(mebibytes):
    return pltpu.CompilerParams(vmem_limit_bytes=mebibytes << 20)


def packed_pair(gate, up, keep):
    aligned = keep // 128 * 128
    pieces = []
    for at in range(0, aligned, 128):
        pieces += [gate[:, at : at + 128], up[:, at : at + 128]]
    if keep > aligned:
        gate_tail, up_tail = gate[:, aligned : aligned + 128], up[:, aligned : aligned + 128]
        lane = lax.broadcasted_iota(jnp.int32, gate_tail.shape, 1)
        pieces.append(jnp.where(lane < keep - aligned, gate_tail, pltpu.roll(up_tail, keep - aligned, 1)))
    return pieces


def pack_kernel(place, gate, up, gate_scale, up_scale, kept, sent, scale):
    keep = kept.shape[1] // 2

    def put(out, gates, ups):
        at = 0
        for piece in packed_pair(gates, ups, keep):
            out[:, at : at + piece.shape[1]] = piece.astype(out.dtype)
            at += piece.shape[1]

    low = (gate[...], up[...])
    high = tuple(pltpu.roll(v, keep, 1) for v in low)
    scales = tuple(jnp.broadcast_to(v[...], (8, 2 * keep)) for v in (gate_scale, up_scale))
    high_scales = tuple(pltpu.roll(v, keep, 1) for v in scales)

    @pl.when(place[1] == 0)
    def _():
        put(kept, *low)
        put(sent, *high)
        put(scale, *scales)

    @pl.when(place[1] != 0)
    def _():
        put(kept, *high)
        put(sent, *low)
        put(scale, *high_scales)


def run_pack(place, gate, up, gate_scale, up_scale):
    rows, width = gate.shape
    both = width // 2
    block = min(rows, 64)
    weight = pl.BlockSpec((block, both), lambda i, p: (i, p[0]))
    scale = pl.BlockSpec((1, both), lambda i, p: (0, p[0]))
    out = pl.BlockSpec((block, both), lambda i, p: (i, 0))
    shape = jax.ShapeDtypeStruct((rows, both), BF)
    return pl.pallas_call(
        pack_kernel,
        grid_spec=pltpu.PrefetchScalarGridSpec(
            num_scalar_prefetch=1,
            grid=(rows // block,),
            in_specs=[weight, weight, scale, scale],
            out_specs=(out, out, pl.BlockSpec((8, both), lambda i, p: (0, 0))),
        ),
        out_shape=(shape, shape, jax.ShapeDtypeStruct((8, both), F32)),
        compiler_params=room(12),
        name="pack",
        cost_estimate=pl.CostEstimate(flops=3_000_000_000, bytes_accessed=5_000_000, transcendentals=0),
    )(place, gate, up, gate_scale, up_scale)


def turn_kernel(place, down, kept, sent):
    keep = kept.shape[0]
    low, high = (down[:, i * keep : (i + 1) * keep].T.astype(BF) for i in range(2))

    @pl.when(place[1] == 0)
    def _():
        kept[...] = low
        sent[...] = high

    @pl.when(place[1] != 0)
    def _():
        kept[...] = high
        sent[...] = low


def run_turn(place, down):
    rows, width = down.shape
    block = 128
    out = pl.BlockSpec((width // 4, block), lambda i, p: (0, i))
    shape = jax.ShapeDtypeStruct((width // 4, rows), BF)
    return pl.pallas_call(
        turn_kernel,
        grid_spec=pltpu.PrefetchScalarGridSpec(
            num_scalar_prefetch=1,
            grid=(rows // block,),
            in_specs=[pl.BlockSpec((block, width // 2), lambda i, p: (i, p[0]))],
            out_specs=(out, out),
        ),
        out_shape=(shape, shape),
        compiler_params=room(12),
        name="turn",
        cost_estimate=pl.CostEstimate(flops=2_000_000_000, bytes_accessed=3_000_000, transcendentals=0),
    )(place, down)


def mixer_kernel(n_ring, half, *refs):
    place, normed, in_scale, mix, mix_scale = refs[:5]
    scales = refs[5 : 5 + n_ring]
    own, other = refs[5 + n_ring : 7 + n_ring]
    rest = refs[7 + n_ring : 7 + n_ring + 4 * (n_ring - 1)]
    part_mine, part_away, weights, packed, sems = refs[7 + n_ring + 4 * (n_ring - 1) :]
    rep, col, core = place[0], place[1], place[2]
    copies = []

    def bring(source, ring, y, h, rows):
        start = pl.multiple_of(ring * 4 * half + y * 2 * half + h * half, half)
        copy = pltpu.make_async_copy(
            source, weights.at[:, pl.ds(start, rows), :], sems.at[len(copies)]
        )
        copy.start()
        copies.append(copy)

    bring(own, 0, col, 0, 2 * half)
    bring(other, 0, 1 - col, 0, 2 * half)
    for k in range(1, n_ring):
        mine, across, beside, corner = rest[4 * (k - 1) : 4 * k]
        bring(mine, k, col, rep, half)
        bring(across, k, col, 1 - rep, half)
        bring(beside, k, 1 - col, rep, half)
        bring(corner, k, 1 - col, 1 - rep, half)
    for copy in copies:
        copy.wait()
    pool_in = jnp.dot(normed[...], weights[0], preferred_element_type=F32)
    pool_in = (pool_in * in_scale[...]).astype(BF)
    length, width = pool_in.shape
    offsets = lax.broadcasted_iota(jnp.int32, (length, length), 0) - lax.broadcasted_iota(
        jnp.int32, (length, length), 1
    )
    places = lax.broadcasted_iota(jnp.int32, (length, 1), 0)
    block = mix.shape[0]
    grouped = []
    for piece in range(width // POOL_GROUP):
        window = lax.shift_left(jnp.int32(2), core * (width // POOL_GROUP) + piece)
        band = jnp.where((offsets >= 0) & (offsets < window), 1.0, 0.0).astype(BF)
        columns = pool_in[:, piece * POOL_GROUP : (piece + 1) * POOL_GROUP]
        sums = jnp.dot(band, columns, preferred_element_type=F32)
        counts = jnp.minimum(places + 1, window).astype(F32)
        pooled = (sums / counts - columns.astype(F32)).astype(BF)
        for b in range(POOL_GROUP // block):
            lo = piece * POOL_GROUP + b * block
            mixed = jnp.dot(
                pooled[:, b * block : (b + 1) * block],
                mix[:, lo : lo + block].astype(BF),
                preferred_element_type=F32,
            )
            grouped.append((mixed * mix_scale[:, lo : lo + block]).astype(BF))
    packed[...] = jnp.concatenate(grouped, axis=1)
    rows = length // 2
    for out, h in ((part_away, 1 - core), (part_mine, core)):
        grouped = packed[pl.ds(pl.multiple_of(h * rows, rows), rows), :]
        for k in range(n_ring):
            for j in range(2):
                y = col if j == 0 else 1 - col
                at = pl.ds(pl.multiple_of((2 * k + y) * 2 * half, 2 * half), 2 * half)
                sums = transposed_product(grouped, weights[1, at, :])
                out[:, at] = (sums * scales[k][j, 0:1, :]).astype(BF)


def run_mixer(place, normed, in_scale, mix, mix_scale, scales, own, other, rest):
    length, width = normed.shape
    half = own.shape[1] // 2
    n_ring = len(scales)
    n_copies = 2 + len(rest)
    shape = jax.ShapeDtypeStruct((length // 2, width), BF)
    return pl.pallas_call(
        functools.partial(mixer_kernel, n_ring, half),
        out_shape=(shape, shape),
        in_specs=[SMEM] + [VMEM] * (4 + n_ring) + [HBM] * n_copies,
        out_specs=(VMEM, VMEM),
        scratch_shapes=[
            pltpu.VMEM((2, width, own.shape[2]), BF),
            pltpu.VMEM((length, own.shape[2]), BF),
            pltpu.SemaphoreType.DMA((n_copies,)),
        ],
        compiler_params=room(24),
        name="mixer",
        cost_estimate=pl.CostEstimate(flops=5_000_000_000, bytes_accessed=10_000_000, transcendentals=512),
    )(place, normed, in_scale, mix, mix_scale, *scales, own, other, *rest)


def normed_rows(floats, gain):
    scaled = floats * lax.rsqrt(jnp.mean(floats * floats, axis=-1, keepdims=True) + epsilon)
    return (scaled * gain).astype(BF)


def turn_into(n_ring, ring, source, out):
    block = out.shape[1] // n_ring
    for k in range(n_ring):
        at = lax.rem(ring - k + n_ring, n_ring) * block
        out[:, k * block : (k + 1) * block] = source[:, pl.ds(pl.multiple_of(at, block), block)]


def ready_kernel(n_ring, place, tokens, gain, next_gain, turned, normed, turned_gain, own_gain):
    turn_into(n_ring, place[3], tokens, turned)
    turn_into(n_ring, place[3], gain, own_gain)
    turn_into(n_ring, place[3], next_gain, turned_gain)
    normed[...] = normed_rows(turned[...].astype(F32), own_gain[...])


def run_ready(place, n_ring, tokens, gain, next_gain):
    length, width = tokens.shape
    block = length // 4
    rows = pl.BlockSpec((block, width), lambda i, p: (i, 0))
    line = pl.BlockSpec((1, width), lambda i, p: (0, 0))
    shape = jax.ShapeDtypeStruct((length, width), BF)
    return pl.pallas_call(
        functools.partial(ready_kernel, n_ring),
        grid_spec=pltpu.PrefetchScalarGridSpec(
            num_scalar_prefetch=1,
            grid=(4,),
            in_specs=[rows, line, line],
            out_specs=(rows, rows, line),
            scratch_shapes=[pltpu.VMEM((1, width), F32)],
        ),
        out_shape=(shape, shape, jax.ShapeDtypeStruct((1, width), F32)),
        compiler_params=room(16),
        name="ready",
        cost_estimate=pl.CostEstimate(flops=3_000_000_000, bytes_accessed=6_000_000, transcendentals=512),
    )(place, tokens, gain, next_gain)


def settle_kernel(place, tokens, part, other, gain, middle_mine, here):
    mixer_out = part[...].astype(F32) + other[...].astype(F32)
    middle = (tokens[...].astype(F32) + mixer_out).astype(BF)
    middle_mine[...] = middle
    here[...] = normed_rows(middle.astype(F32), gain[...])


def run_settle(place, tokens, part, other, gain):
    rows, width = part.shape
    block = rows // 4
    shape = jax.ShapeDtypeStruct((rows, width), BF)
    spec = pl.BlockSpec((block, width), lambda i, p: (i, 0))
    return pl.pallas_call(
        settle_kernel,
        grid_spec=pltpu.PrefetchScalarGridSpec(
            num_scalar_prefetch=1,
            grid=(4,),
            in_specs=[
                pl.BlockSpec((block, width), lambda i, p: (p[2] * 4 + i, 0)), spec, spec,
                pl.BlockSpec((1, width), lambda i, p: (0, 0)),
            ],
            out_specs=(spec, spec),
        ),
        out_shape=(shape, shape),
        compiler_params=room(16),
        name="settle",
        cost_estimate=pl.CostEstimate(flops=3_000_000_000, bytes_accessed=9_000_000, transcendentals=512),
    )(place, tokens, part, other, gain)


def gated_kernel(n_rows, starts, n_weights, *refs):
    place, scale, other_scale = refs[:3]
    rows = refs[3 : 3 + n_rows]
    parts = refs[3 + n_rows : 3 + n_rows + n_weights]
    hidden, weights, stage, row_sems, sems = refs[3 + n_rows + n_weights :]
    shard, both = parts[0].shape
    keep = both // 2
    aligned = keep // 128 * 128
    tail = keep - aligned
    batches = ([], [], [])
    for i, p in enumerate(parts):
        y = place[1] if i // 2 % 2 == 0 else 1 - place[1]
        at = pl.ds(pl.multiple_of((i // 4 * 2 + y) * shard, shard), shard)
        main, end = i % 2 * 2 * aligned, 4 * aligned + i % 2 * 2 * tail
        for batch, start, to, size in ((i % 2, 0, main, 2 * aligned), (2, 2 * aligned, end, 2 * tail)):
            if size:
                batches[batch].append(
                    pltpu.make_async_copy(
                        p.at[:, pl.ds(start, size)], weights.at[at, pl.ds(to, size)],
                        sems.at[2 * i + batch // 2],
                    )
                )
    row_copies = [
        pltpu.make_async_copy(r, stage.at[pl.ds(start, r.shape[0]), :], row_sems.at[i])
        for i, (r, start) in enumerate(zip(rows, starts))
    ]
    for batch in (row_copies, *batches):
        for copy in batch:
            copy.start()
    for copy in row_copies:
        copy.wait()

    def product(lo, size):
        return jnp.dot(stage[...], weights[:, lo : lo + size], preferred_element_type=F32)

    for j, line in enumerate((scale, other_scale)):
        for copy in batches[j]:
            copy.wait()
        for at in range(0, aligned, 128):
            sums = product(2 * (j * aligned + at), 256) * line[0:1, 2 * at : 2 * at + 256]
            gate, up = sums[:, :128], sums[:, 128:]
            hidden[:, j * aligned + at : j * aligned + at + 128] = (jax.nn.silu(gate) * up).astype(BF)
    if tail:
        for copy in batches[2]:
            copy.wait()
        sums = product(4 * aligned, 4 * tail)
        own, other = (
            sums[:, 2 * j * tail : 2 * (j + 1) * tail] * line[0:1, 2 * aligned :]
            for j, line in enumerate((scale, other_scale))
        )
        lane = lax.broadcasted_iota(jnp.int32, own.shape, 1)
        gate = jnp.where(lane < tail, own, pltpu.roll(other, tail, 1))
        up = jnp.where(lane < tail, pltpu.roll(own, tail, 1), other)
        hidden[:, 2 * aligned :] = (jax.nn.silu(gate) * up).astype(BF)


def run_gated(place, scale, other_scale, rows, parts):
    starts, total = [], 0
    for r in rows:
        starts.append(total)
        total += r.shape[0]
    width = rows[0].shape[1]
    both = parts[0].shape[1]
    return pl.pallas_call(
        functools.partial(gated_kernel, len(rows), tuple(starts), len(parts)),
        out_shape=jax.ShapeDtypeStruct((total, both), BF),
        in_specs=[SMEM, VMEM, VMEM] + [HBM] * (len(rows) + len(parts)),
        out_specs=VMEM,
        scratch_shapes=[
            pltpu.VMEM((width, 2 * both), BF),
            pltpu.VMEM((total, width), BF),
            pltpu.SemaphoreType.DMA((len(rows),)),
            pltpu.SemaphoreType.DMA((2 * len(parts),)),
        ],
        compiler_params=room(34),
        name="gated",
        cost_estimate=pl.CostEstimate(flops=12_000_000_000, bytes_accessed=20_000_000, transcendentals=1_500_000),
    )(place, scale, other_scale, *rows, *parts)


def keep_kernel(k, place, hidden, scale, middle, *refs):
    both, both_other, base = refs[:3]
    outs, ends = refs[3:6], refs[6]
    _, keep, width = both.shape
    aligned = keep // 128 * 128
    tail = keep - aligned
    rows = base.shape[0]
    for i in range(2):
        own, other = both.at[i], both_other.at[i]
        y = place[1] if i == 0 else 1 - place[1]
        lanes = pl.ds(pl.multiple_of(y * width, width), width)
        from_lanes = pl.ds(pl.multiple_of((2 * k + y) * width, width), width)
        ends[:tail, :] = own[aligned:, :]
        ends[tail:, :] = other[aligned:, :]
        total = jnp.dot(hidden[:, :aligned], own[:aligned, :], preferred_element_type=F32)
        total += jnp.dot(
            hidden[:, aligned : 2 * aligned], other[:aligned, :], preferred_element_type=F32
        )
        total += jnp.dot(hidden[:, 2 * aligned :], ends[...], preferred_element_type=F32)
        total = total * scale[i, 1:2, :]
        base[:, lanes] = total[:rows, :] + middle[:, from_lanes].astype(F32)
        for j, out in enumerate(outs):
            out[:, lanes] = total[(j + 1) * rows : (j + 2) * rows, :].astype(BF)


def run_keep(place, hidden, scale, middle, parts, k):
    rows = hidden.shape[0] // 4
    _, keep, width = parts[0].shape
    shape = jax.ShapeDtypeStruct((rows, 2 * width), BF)
    return pl.pallas_call(
        functools.partial(keep_kernel, k),
        in_specs=[SMEM] + [VMEM] * 5,
        out_specs=(VMEM, VMEM, VMEM, VMEM),
        scratch_shapes=[pltpu.VMEM((2 * (keep % 128), width), BF)],
        out_shape=(jax.ShapeDtypeStruct(shape.shape, F32), shape, shape, shape),
        compiler_params=room(20),
        name="keep",
        cost_estimate=pl.CostEstimate(flops=2_000_000_000, bytes_accessed=5_000_000, transcendentals=0),
    )(place, hidden, scale, middle, *parts)


def join_kernel(base, first, second, third, out):
    total = base[...] + first[...].astype(F32) + second[...].astype(F32) + third[...].astype(F32)
    out[...] = total.astype(BF)


def run_join(base, *others):
    return pl.pallas_call(
        join_kernel,
        in_specs=[VMEM] * 4,
        out_specs=VMEM,
        out_shape=jax.ShapeDtypeStruct(base.shape, BF),
        compiler_params=room(8),
        name="join",
        cost_estimate=pl.CostEstimate(flops=1_000_000_000, bytes_accessed=2_000_000, transcendentals=0),
    )(base, *others)


def collect_kernel(n_ring, steps, *refs):
    place = refs[0]
    pieces = refs[1 : 1 + 2 * len(steps)]
    out, sems = refs[-2:]
    rows, width = pieces[0].shape
    copies = []
    for i, piece in enumerate(pieces):
        h = place[2] if i % 2 == 0 else 1 - place[2]
        block = lax.rem(place[3] - steps[i // 2] + n_ring, n_ring)
        at = out.at[
            pl.ds(pl.multiple_of(h * rows, rows), rows),
            pl.ds(pl.multiple_of(block * width, width), width),
        ]
        copy = pltpu.make_async_copy(piece, at, sems.at[i])
        copy.start()
        copies.append(copy)
    for copy in copies:
        copy.wait()


def run_collect(place, n_ring, steps, pieces, into=None):
    rows, width = pieces[0].shape
    extra = [] if into is None else [into]
    return pl.pallas_call(
        functools.partial(collect_kernel, n_ring, steps),
        out_shape=jax.ShapeDtypeStruct((2 * rows, width * n_ring), BF),
        in_specs=[SMEM] + [VMEM] * len(pieces) + [HBM] * len(extra),
        out_specs=HBM,
        input_output_aliases={1 + len(pieces): 0} if extra else {},
        scratch_shapes=[pltpu.SemaphoreType.DMA((len(pieces),))],
        compiler_params=room(12),
        name="collect",
        cost_estimate=pl.CostEstimate(flops=2_000_000_000, bytes_accessed=4_000_000, transcendentals=0),
    )(place, *pieces, *extra)


def shared_body(
    n_fs,
    tokens, mixer_gain, pool_input, input_scale, group_mix, group_scale, pool_output, output_scale,
    channel_gain, gate_weight, gate_scale, up_weight, up_scale, down_weight, down_scale,
):
    n_ring = n_fs // 2
    rep, fs, core = lax.axis_index("rep"), lax.axis_index("fs"), lax.axis_index("tp")
    ring, col = fs // 2, fs % 2
    half = pool_input.shape[0] // 2
    rows = tokens.shape[0] // 2

    swap = [(0, 1), (1, 0)]
    col_swap = [(i, i ^ 1) for i in range(n_fs)]
    diagonal = [
        (a * n_fs + i, (1 - a) * n_fs + (i ^ 1)) for a in range(2) for i in range(n_fs)
    ]

    def across(value):
        return lax.ppermute(value, "rep", swap)

    def beside(value):
        return lax.ppermute(value, "fs", col_swap)

    def corner(value):
        return lax.ppermute(value, ("rep", "fs"), diagonal)

    def partner(value):
        return lax.ppermute(value, "tp", swap)

    def around(value, steps=1):
        return lax.ppermute(
            value, "fs", [(i, (i + 2 * steps) % n_fs) for i in range(n_fs)]
        )

    place = jnp.stack([rep, col, core, ring]).astype(jnp.int32)

    own = jnp.stack([pool_input.astype(BF), pool_output.astype(BF)])
    mine = [lax.dynamic_slice_in_dim(own, rep * half, half, axis=1)]
    mine += [around(mine[0])]
    mine += [around(mine[1], k - 1) for k in range(2, n_ring - 1)]
    mine += [around(mine[0], -1)]
    other = beside(own)
    rest = []
    for k in range(1, n_ring):
        next_to, facing = beside(mine[k]), across(mine[k])
        last = across(next_to)
        rest += [mine[k], facing, next_to, last]

    own_scale = jnp.stack([output_scale, down_scale])
    pair = jnp.stack([own_scale, beside(own_scale)])
    scales = [pair] + [around(pair, k) for k in range(1, n_ring)]

    def circled(start, back):
        chain = [start, around(start)]
        for _ in range(2, n_ring - back):
            chain.append(around(chain[-1]))
        if back:
            chain.append(around(start, -1))
        return [(c, partner(c)) for c in chain]

    gated_kept, gated_sent, gated_scale = run_pack(place, gate_weight, up_weight, gate_scale[None], up_scale[None])
    own_column, next_column = circled(gated_kept, 0), circled(beside(gated_sent), 0)
    gated_parts = [a + b for a, b in zip(own_column, next_column)]
    down_kept, down_sent = run_turn(place, down_weight)
    down_parts = circled(jnp.stack([down_kept, beside(down_sent)]), 1)

    tokens, normed, next_gain = run_ready(place, n_ring, tokens, mixer_gain[None], channel_gain[None])
    part_mine, part_away = run_mixer(
        place, normed, input_scale[None], group_mix, group_scale[None], scales, own,
        other, rest,
    )
    middle_mine, here = run_settle(place, tokens, part_mine, partner(part_away), next_gain)

    ax, ay = across(here), beside(here)
    cut = rows // 2
    far = [across(ay[:cut]), beside(ax[cut:])]
    hidden = run_gated(
        place, gated_scale, partner(gated_scale), [here, ax, ay] + far,
        sum(gated_parts, ()),
    )

    pieces = []
    steps = (0, 1) + tuple(range(n_ring - 1, 1, -1))
    for k in steps:
        base, to_x, to_y, to_far = run_keep(place, hidden, scales[k], middle_mine, down_parts[k], k)
        total = run_join(
            base, across(to_x), beside(to_y),
            corner(to_far),
        )
        pieces.append((total, partner(total)))
    early = run_collect(place, n_ring, steps[:-1], sum(pieces[:-1], ()))
    return run_collect(place, n_ring, steps[-1:], pieces[-1], early)


def solution(mesh):
    in_specs = (
        P(("rep", "fs"), None), P(), P("fs", "tp"), P("tp"), P(None, "tp"), P("tp"), P("fs", "tp"),
        P("fs"), P(), P("fs", "tp"), P("tp"), P("fs", "tp"), P("tp"), P("fs", "tp"), P("fs"),
    )
    out_specs = P(("rep", "fs"), None)
    n_rep, n_fs, n_tp = (mesh.shape[a] for a in ("rep", "fs", "tp"))
    shared = n_rep == 2 and n_tp == 2 and n_fs == 8

    def body(*args):
        return shared_body(n_fs, *args) if shared else plain_body(*args)

    return jax.shard_map(body, mesh=mesh, in_specs=in_specs, out_specs=out_specs, check_vma=False)
```

```python
import functools
import jax
import jax.numpy as jnp
from jax import lax
from jax.experimental import pallas as pl
from jax.experimental.pallas import tpu as pltpu
from jax.sharding import PartitionSpec as P


POOL_GROUP = 256
BF = jnp.bfloat16
F32 = jnp.float32
epsilon = 1e-06


def rms_norm(row_block, gain_row):
    floats = row_block.astype(F32)
    scaled = floats * lax.rsqrt(jnp.mean(floats * floats, axis=-1, keepdims=True) + epsilon)
    return (scaled * gain_row).astype(BF)


def transposed_product(left_rows, weight_rows):
    return lax.dot_general(
        left_rows, weight_rows, (((1,), (1,)), ((), ())), preferred_element_type=F32
    )


def plain_body(
    tokens, mixer_gain, pool_input, input_scale, group_mix, group_scale, pool_output, output_scale,
    channel_gain, gate_weight, gate_scale, up_weight, up_scale, down_weight, down_scale,
):
    def gather(value):
        return lax.all_gather(value, "fs", axis=0, tiled=True)

    length = tokens.shape[0]
    block_width, local_width = group_mix.shape
    normed = rms_norm(tokens, mixer_gain)
    input_full = gather(pool_input.astype(BF))
    output_full = gather(pool_output.astype(BF))
    output_feature, down_feature = gather(output_scale), gather(down_scale)
    pool_in = (jnp.dot(normed, input_full, preferred_element_type=F32) * input_scale).astype(BF)
    places = jnp.arange(length, dtype=jnp.int32)
    offsets = places[:, None] - places[None, :]
    chunk = min(POOL_GROUP, local_width)
    pieces = []
    for piece in range(local_width // chunk):
        group_index = (lax.axis_index("tp") * local_width + piece * chunk) // POOL_GROUP
        window = lax.shift_left(jnp.int32(2), group_index.astype(jnp.int32))
        band_mask = ((offsets >= 0) & (offsets < window)).astype(BF)
        columns = pool_in[:, piece * chunk : (piece + 1) * chunk]
        window_sums = jnp.dot(band_mask, columns, preferred_element_type=F32)
        counts = jnp.minimum(places + 1, window).astype(F32)
        pieces.append((window_sums / counts[:, None] - columns.astype(F32)).astype(BF))
    pooled = jnp.concatenate(pieces, axis=1)
    local_blocks = local_width // block_width
    mixed_raw = jnp.einsum(
        "sgc,cgd->sgd",
        pooled.reshape(length, local_blocks, block_width),
        group_mix.astype(BF).reshape(block_width, local_blocks, block_width),
        preferred_element_type=F32,
    ).reshape(length, local_width)
    grouped = (mixed_raw * group_scale).astype(BF)
    partial_value = (transposed_product(grouped, output_full) * output_feature).astype(BF)
    mixer_out = lax.psum(partial_value, "tp").astype(F32)
    middle = (tokens.astype(F32) + mixer_out).astype(BF)
    second = rms_norm(middle, channel_gain)
    gate_sum = jnp.dot(second, gather(gate_weight.astype(BF)), preferred_element_type=F32)
    up_sum = jnp.dot(second, gather(up_weight.astype(BF)), preferred_element_type=F32)
    hidden = (jax.nn.silu(gate_sum * gate_scale) * (up_sum * up_scale)).astype(BF)
    projected = transposed_product(hidden, gather(down_weight.astype(BF)))
    channel_part = (projected * down_feature).astype(BF)
    channel_out = lax.psum(channel_part, "tp").astype(F32)
    return (middle.astype(F32) + channel_out).astype(BF)


VMEM = pl.BlockSpec(memory_space=pltpu.VMEM)
SMEM = pl.BlockSpec(memory_space=pltpu.SMEM)
HBM = pl.BlockSpec(memory_space=pltpu.HBM)


def room(mebibytes):
    return pltpu.CompilerParams(vmem_limit_bytes=mebibytes << 20)


def packed_pair(gate, up, keep):
    aligned = keep // 128 * 128
    pieces = []
    for at in range(0, aligned, 128):
        pieces += [gate[:, at : at + 128], up[:, at : at + 128]]
    if keep > aligned:
        gate_tail, up_tail = gate[:, aligned : aligned + 128], up[:, aligned : aligned + 128]
        lane = lax.broadcasted_iota(jnp.int32, gate_tail.shape, 1)
        pieces.append(jnp.where(lane < keep - aligned, gate_tail, pltpu.roll(up_tail, keep - aligned, 1)))
    return pieces


def pack_kernel(place, gate, up, gate_scale, up_scale, kept, kept_late, sent, sent_late, scale):
    keep = scale.shape[1] // 2
    cut = kept.shape[1]

    def put(outs, gates, ups):
        at = 0
        for piece in packed_pair(gates, ups, keep):
            out, to = (outs[1], at - cut) if at >= cut and len(outs) > 1 else (outs[0], at)
            out[:, to : to + piece.shape[1]] = piece.astype(out.dtype)
            at += piece.shape[1]

    low = (gate[...], up[...])
    high = tuple(pltpu.roll(v, keep, 1) for v in low)
    scales = tuple(jnp.broadcast_to(v[...], (8, 2 * keep)) for v in (gate_scale, up_scale))
    high_scales = tuple(pltpu.roll(v, keep, 1) for v in scales)

    @pl.when(place[1] == 0)
    def _():
        put((kept, kept_late), *low)
        put((sent, sent_late), *high)
        put((scale,), *scales)

    @pl.when(place[1] != 0)
    def _():
        put((kept, kept_late), *high)
        put((sent, sent_late), *low)
        put((scale,), *high_scales)


def run_pack(place, gate, up, gate_scale, up_scale):
    rows, width = gate.shape
    both = width // 2
    block = min(rows, 64)
    weight = pl.BlockSpec((block, both), lambda i, p: (i, p[0]))
    scale = pl.BlockSpec((1, both), lambda i, p: (0, p[0]))
    cut = (both // 256 + 1) // 2 * 256
    outs = [pl.BlockSpec((block, c), lambda i, p: (i, 0)) for c in (cut, both - cut)] * 2
    shapes = [jax.ShapeDtypeStruct((rows, c), BF) for c in (cut, both - cut)] * 2
    return pl.pallas_call(
        pack_kernel,
        grid_spec=pltpu.PrefetchScalarGridSpec(
            num_scalar_prefetch=1,
            grid=(rows // block,),
            in_specs=[weight, weight, scale, scale],
            out_specs=(*outs, pl.BlockSpec((8, both), lambda i, p: (0, 0))),
        ),
        out_shape=(*shapes, jax.ShapeDtypeStruct((8, both), F32)),
        compiler_params=room(12),
        name="pack",
        cost_estimate=pl.CostEstimate(flops=3_000_000_000, bytes_accessed=5_000_000, transcendentals=0),
    )(place, gate, up, gate_scale, up_scale)


def turn_kernel(place, down, kept, sent):
    keep = kept.shape[0]
    low, high = (down[:, i * keep : (i + 1) * keep].T.astype(BF) for i in range(2))

    @pl.when(place[1] == 0)
    def _():
        kept[...] = low
        sent[...] = high

    @pl.when(place[1] != 0)
    def _():
        kept[...] = high
        sent[...] = low


def run_turn(place, down):
    rows, width = down.shape
    block = 128
    out = pl.BlockSpec((width // 4, block), lambda i, p: (0, i))
    shape = jax.ShapeDtypeStruct((width // 4, rows), BF)
    return pl.pallas_call(
        turn_kernel,
        grid_spec=pltpu.PrefetchScalarGridSpec(
            num_scalar_prefetch=1,
            grid=(rows // block,),
            in_specs=[pl.BlockSpec((block, width // 2), lambda i, p: (i, p[0]))],
            out_specs=(out, out),
        ),
        out_shape=(shape, shape),
        compiler_params=room(12),
        name="turn",
        cost_estimate=pl.CostEstimate(flops=2_000_000_000, bytes_accessed=3_000_000, transcendentals=0),
    )(place, down)


def mixer_kernel(n_ring, half, *refs):
    place, normed, in_scale, mix, mix_scale = refs[:5]
    scales = refs[5 : 5 + n_ring]
    own, other = refs[5 + n_ring : 7 + n_ring]
    rest = refs[7 + n_ring : 7 + n_ring + 4 * (n_ring - 1)]
    part_mine, part_away, weights, packed, sems = refs[7 + n_ring + 4 * (n_ring - 1) :]
    rep, col, core = place[0], place[1], place[2]
    copies = []

    def bring(source, ring, y, h, rows):
        start = pl.multiple_of(ring * 4 * half + y * 2 * half + h * half, half)
        copy = pltpu.make_async_copy(
            source, weights.at[:, pl.ds(start, rows), :], sems.at[len(copies)]
        )
        copy.start()
        copies.append(copy)

    bring(own, 0, col, 0, 2 * half)
    bring(other, 0, 1 - col, 0, 2 * half)
    for k in range(1, n_ring):
        mine, across, beside, corner = rest[4 * (k - 1) : 4 * k]
        bring(mine, k, col, rep, half)
        bring(across, k, col, 1 - rep, half)
        bring(beside, k, 1 - col, rep, half)
        bring(corner, k, 1 - col, 1 - rep, half)
    for copy in copies:
        copy.wait()
    pool_in = jnp.dot(normed[...], weights[0], preferred_element_type=F32)
    pool_in = (pool_in * in_scale[...]).astype(BF)
    length, width = pool_in.shape
    offsets = lax.broadcasted_iota(jnp.int32, (length, length), 0) - lax.broadcasted_iota(
        jnp.int32, (length, length), 1
    )
    places = lax.broadcasted_iota(jnp.int32, (length, 1), 0)
    block = mix.shape[0]
    grouped = []
    for piece in range(width // POOL_GROUP):
        window = lax.shift_left(jnp.int32(2), core * (width // POOL_GROUP) + piece)
        band = jnp.where((offsets >= 0) & (offsets < window), 1.0, 0.0).astype(BF)
        columns = pool_in[:, piece * POOL_GROUP : (piece + 1) * POOL_GROUP]
        sums = jnp.dot(band, columns, preferred_element_type=F32)
        counts = jnp.minimum(places + 1, window).astype(F32)
        pooled = (sums / counts - columns.astype(F32)).astype(BF)
        for b in range(POOL_GROUP // block):
            lo = piece * POOL_GROUP + b * block
            mixed = jnp.dot(
                pooled[:, b * block : (b + 1) * block],
                mix[:, lo : lo + block].astype(BF),
                preferred_element_type=F32,
            )
            grouped.append((mixed * mix_scale[:, lo : lo + block]).astype(BF))
    packed[...] = jnp.concatenate(grouped, axis=1)
    rows = length // 2
    for out, h in ((part_away, 1 - core), (part_mine, core)):
        grouped = packed[pl.ds(pl.multiple_of(h * rows, rows), rows), :]
        for k in range(n_ring):
            for j in range(2):
                y = col if j == 0 else 1 - col
                at = pl.ds(pl.multiple_of((2 * k + y) * 2 * half, 2 * half), 2 * half)
                sums = transposed_product(grouped, weights[1, at, :])
                out[:, at] = (sums * scales[k][j, 0:1, :]).astype(BF)


def run_mixer(place, normed, in_scale, mix, mix_scale, scales, own, other, rest):
    length, width = normed.shape
    half = own.shape[1] // 2
    n_ring = len(scales)
    n_copies = 2 + len(rest)
    shape = jax.ShapeDtypeStruct((length // 2, width), BF)
    return pl.pallas_call(
        functools.partial(mixer_kernel, n_ring, half),
        out_shape=(shape, shape),
        in_specs=[SMEM] + [VMEM] * (4 + n_ring) + [HBM] * n_copies,
        out_specs=(VMEM, VMEM),
        scratch_shapes=[
            pltpu.VMEM((2, width, own.shape[2]), BF),
            pltpu.VMEM((length, own.shape[2]), BF),
            pltpu.SemaphoreType.DMA((n_copies,)),
        ],
        compiler_params=room(24),
        name="mixer",
        cost_estimate=pl.CostEstimate(flops=5_000_000_000, bytes_accessed=10_000_000, transcendentals=512),
    )(place, normed, in_scale, mix, mix_scale, *scales, own, other, *rest)


def normed_rows(floats, gain):
    scaled = floats * lax.rsqrt(jnp.mean(floats * floats, axis=-1, keepdims=True) + epsilon)
    return (scaled * gain).astype(BF)


def turn_into(n_ring, ring, source, out):
    block = out.shape[1] // n_ring
    for k in range(n_ring):
        at = lax.rem(ring - k + n_ring, n_ring) * block
        out[:, k * block : (k + 1) * block] = source[:, pl.ds(pl.multiple_of(at, block), block)]


def ready_kernel(n_ring, place, tokens, gain, next_gain, turned, normed, turned_gain, own_gain):
    turn_into(n_ring, place[3], tokens, turned)
    turn_into(n_ring, place[3], gain, own_gain)
    turn_into(n_ring, place[3], next_gain, turned_gain)
    normed[...] = normed_rows(turned[...].astype(F32), own_gain[...])


def run_ready(place, n_ring, tokens, gain, next_gain):
    length, width = tokens.shape
    block = length // 4
    rows = pl.BlockSpec((block, width), lambda i, p: (i, 0))
    line = pl.BlockSpec((1, width), lambda i, p: (0, 0))
    shape = jax.ShapeDtypeStruct((length, width), BF)
    return pl.pallas_call(
        functools.partial(ready_kernel, n_ring),
        grid_spec=pltpu.PrefetchScalarGridSpec(
            num_scalar_prefetch=1,
            grid=(4,),
            in_specs=[rows, line, line],
            out_specs=(rows, rows, line),
            scratch_shapes=[pltpu.VMEM((1, width), F32)],
        ),
        out_shape=(shape, shape, jax.ShapeDtypeStruct((1, width), F32)),
        compiler_params=room(16),
        name="ready",
        cost_estimate=pl.CostEstimate(flops=3_000_000_000, bytes_accessed=6_000_000, transcendentals=512),
    )(place, tokens, gain, next_gain)


def settle_kernel(place, tokens, part, other, gain, middle_mine, here):
    mixer_out = part[...].astype(F32) + other[...].astype(F32)
    middle = (tokens[...].astype(F32) + mixer_out).astype(BF)
    middle_mine[...] = middle
    here[...] = normed_rows(middle.astype(F32), gain[...])


def run_settle(place, tokens, part, other, gain):
    rows, width = part.shape
    block = rows // 4
    shape = jax.ShapeDtypeStruct((rows, width), BF)
    spec = pl.BlockSpec((block, width), lambda i, p: (i, 0))
    return pl.pallas_call(
        settle_kernel,
        grid_spec=pltpu.PrefetchScalarGridSpec(
            num_scalar_prefetch=1,
            grid=(4,),
            in_specs=[
                pl.BlockSpec((block, width), lambda i, p: (p[2] * 4 + i, 0)), spec, spec,
                pl.BlockSpec((1, width), lambda i, p: (0, 0)),
            ],
            out_specs=(spec, spec),
        ),
        out_shape=(shape, shape),
        compiler_params=room(16),
        name="settle",
        cost_estimate=pl.CostEstimate(flops=3_000_000_000, bytes_accessed=9_000_000, transcendentals=512),
    )(place, tokens, part, other, gain)


def gated_kernel(offset, n_rows, starts, n_weights, *refs):
    place, scale, other_scale = refs[:3]
    rows = refs[3 : 3 + n_rows]
    parts = refs[3 + n_rows : 3 + n_rows + n_weights]
    if starts:
        hidden, stage, weights, row_sems, sems = refs[3 + n_rows + n_weights :]
    else:
        hidden, weights, row_sems, sems = refs[3 + n_rows + n_weights :]
        stage = rows[0]
    shard, both = parts[0].shape
    keep = both // 2
    aligned = keep // 128 * 128
    tail = keep - aligned
    batches = ([], [], [])
    for i, p in enumerate(parts):
        y = place[1] if i // 2 % 2 == 0 else 1 - place[1]
        at = pl.ds(pl.multiple_of((i // 4 * 2 + y) * shard, shard), shard)
        main, end = i % 2 * 2 * aligned, 4 * aligned + i % 2 * 2 * tail
        for batch, start, to, size in ((i % 2, 0, main, 2 * aligned), (2, 2 * aligned, end, 2 * tail)):
            if size:
                batches[batch].append(
                    pltpu.make_async_copy(
                        p.at[:, pl.ds(start, size)], weights.at[at, pl.ds(to, size)],
                        sems.at[2 * i + batch // 2],
                    )
                )
    row_copies = [
        pltpu.make_async_copy(r, stage.at[pl.ds(start, r.shape[0]), :], row_sems.at[i])
        for i, (r, start) in enumerate(zip(rows, starts))
    ]
    for batch in (row_copies, *batches):
        for copy in batch:
            copy.start()
    for copy in row_copies:
        copy.wait()

    def product(lo, size):
        return jnp.dot(stage[...], weights[:, lo : lo + size], preferred_element_type=F32)

    for j, line in enumerate((scale, other_scale)):
        for copy in batches[j]:
            copy.wait()
        for at in range(0, aligned, 128):
            sums = product(2 * (j * aligned + at), 256) * line[0:1, offset + 2 * at : offset + 2 * at + 256]
            gate, up = sums[:, :128], sums[:, 128:]
            hidden[:, j * aligned + at : j * aligned + at + 128] = (jax.nn.silu(gate) * up).astype(BF)
    if tail:
        for copy in batches[2]:
            copy.wait()
        sums = product(4 * aligned, 4 * tail)
        own, other = (
            sums[:, 2 * j * tail : 2 * (j + 1) * tail] * line[0:1, offset + 2 * aligned :]
            for j, line in enumerate((scale, other_scale))
        )
        lane = lax.broadcasted_iota(jnp.int32, own.shape, 1)
        gate = jnp.where(lane < tail, own, pltpu.roll(other, tail, 1))
        up = jnp.where(lane < tail, pltpu.roll(own, tail, 1), other)
        hidden[:, 2 * aligned :] = (jax.nn.silu(gate) * up).astype(BF)


def run_gated(place, scale, other_scale, rows, parts, offset):
    starts, total = [], 0
    for r in rows:
        starts.append(total)
        total += r.shape[0]
    gathers = len(rows) > 1
    width = rows[0].shape[1]
    both = parts[0].shape[1]
    shapes = [jax.ShapeDtypeStruct((total, both), BF), jax.ShapeDtypeStruct((total, width), BF)]
    return pl.pallas_call(
        functools.partial(
            gated_kernel, offset, len(rows), tuple(starts) if gathers else (), len(parts)
        ),
        out_shape=tuple(shapes) if gathers else shapes[0],
        in_specs=[SMEM, VMEM, VMEM] + [HBM if gathers else VMEM] * len(rows) + [HBM] * len(parts),
        out_specs=(VMEM, VMEM) if gathers else VMEM,
        scratch_shapes=[
            pltpu.VMEM((width, 2 * both), BF),
            pltpu.SemaphoreType.DMA((len(rows),)),
            pltpu.SemaphoreType.DMA((2 * len(parts),)),
        ],
        compiler_params=room(24),
        name="gated",
        cost_estimate=pl.CostEstimate(flops=6_000_000_000, bytes_accessed=12_000_000, transcendentals=700_000),
    )(place, scale, other_scale, *rows, *parts)


def keep_kernel(k, place, early, late, scale, middle, *refs):
    both, both_other, base = refs[:3]
    outs, ends = refs[3:6], refs[6]
    _, keep, width = both.shape
    aligned = keep // 128 * 128
    tail = keep - aligned
    cut = early.shape[1] // 2
    rows = base.shape[0]
    for i in range(2):
        own, other = both.at[i], both_other.at[i]
        y = place[1] if i == 0 else 1 - place[1]
        lanes = pl.ds(pl.multiple_of(y * width, width), width)
        from_lanes = pl.ds(pl.multiple_of((2 * k + y) * width, width), width)
        ends[:tail, :] = own[aligned:, :]
        ends[tail:, :] = other[aligned:, :]
        total = jnp.dot(late[:, 2 * (aligned - cut) :], ends[...], preferred_element_type=F32)
        for j, weight in enumerate((own, other)):
            total += jnp.dot(
                early[:, j * cut : (j + 1) * cut], weight[:cut, :], preferred_element_type=F32
            )
            total += jnp.dot(
                late[:, j * (aligned - cut) : (j + 1) * (aligned - cut)], weight[cut:aligned, :],
                preferred_element_type=F32,
            )
        total = total * scale[i, 1:2, :]
        base[:, lanes] = total[:rows, :] + middle[:, from_lanes].astype(F32)
        for j, out in enumerate(outs):
            out[:, lanes] = total[(j + 1) * rows : (j + 2) * rows, :].astype(BF)


def run_keep(place, early, late, scale, middle, parts, k):
    rows = early.shape[0] // 4
    _, keep, width = parts[0].shape
    shape = jax.ShapeDtypeStruct((rows, 2 * width), BF)
    return pl.pallas_call(
        functools.partial(keep_kernel, k),
        in_specs=[SMEM] + [VMEM] * 6,
        out_specs=(VMEM, VMEM, VMEM, VMEM),
        scratch_shapes=[pltpu.VMEM((2 * (keep % 128), width), BF)],
        out_shape=(jax.ShapeDtypeStruct(shape.shape, F32), shape, shape, shape),
        compiler_params=room(20),
        name="keep",
        cost_estimate=pl.CostEstimate(flops=2_000_000_000, bytes_accessed=5_000_000, transcendentals=0),
    )(place, early, late, scale, middle, *parts)


def join_kernel(base, first, second, third, out):
    total = base[...] + first[...].astype(F32) + second[...].astype(F32) + third[...].astype(F32)
    out[...] = total.astype(BF)


def run_join(base, *others):
    return pl.pallas_call(
        join_kernel,
        in_specs=[VMEM] * 4,
        out_specs=VMEM,
        out_shape=jax.ShapeDtypeStruct(base.shape, BF),
        compiler_params=room(8),
        name="join",
        cost_estimate=pl.CostEstimate(flops=1_000_000_000, bytes_accessed=2_000_000, transcendentals=0),
    )(base, *others)


def collect_kernel(n_ring, steps, *refs):
    place = refs[0]
    pieces = refs[1 : 1 + 2 * len(steps)]
    out, sems = refs[-2:]
    rows, width = pieces[0].shape
    copies = []
    for i, piece in enumerate(pieces):
        h = place[2] if i % 2 == 0 else 1 - place[2]
        block = lax.rem(place[3] - steps[i // 2] + n_ring, n_ring)
        at = out.at[
            pl.ds(pl.multiple_of(h * rows, rows), rows),
            pl.ds(pl.multiple_of(block * width, width), width),
        ]
        copy = pltpu.make_async_copy(piece, at, sems.at[i])
        copy.start()
        copies.append(copy)
    for copy in copies:
        copy.wait()


def run_collect(place, n_ring, steps, pieces, into=None):
    rows, width = pieces[0].shape
    extra = [] if into is None else [into]
    return pl.pallas_call(
        functools.partial(collect_kernel, n_ring, steps),
        out_shape=jax.ShapeDtypeStruct((2 * rows, width * n_ring), BF),
        in_specs=[SMEM] + [VMEM] * len(pieces) + [HBM] * len(extra),
        out_specs=HBM,
        input_output_aliases={1 + len(pieces): 0} if extra else {},
        scratch_shapes=[pltpu.SemaphoreType.DMA((len(pieces),))],
        compiler_params=room(12),
        name="collect",
        cost_estimate=pl.CostEstimate(flops=2_000_000_000, bytes_accessed=4_000_000, transcendentals=0),
    )(place, *pieces, *extra)


def shared_body(
    n_fs,
    tokens, mixer_gain, pool_input, input_scale, group_mix, group_scale, pool_output, output_scale,
    channel_gain, gate_weight, gate_scale, up_weight, up_scale, down_weight, down_scale,
):
    n_ring = n_fs // 2
    rep, fs, core = lax.axis_index("rep"), lax.axis_index("fs"), lax.axis_index("tp")
    ring, col = fs // 2, fs % 2
    half = pool_input.shape[0] // 2
    rows = tokens.shape[0] // 2

    swap = [(0, 1), (1, 0)]
    col_swap = [(i, i ^ 1) for i in range(n_fs)]
    diagonal = [
        (a * n_fs + i, (1 - a) * n_fs + (i ^ 1)) for a in range(2) for i in range(n_fs)
    ]

    def across(value):
        return lax.ppermute(value, "rep", swap)

    def beside(value):
        return lax.ppermute(value, "fs", col_swap)

    def corner(value):
        return lax.ppermute(value, ("rep", "fs"), diagonal)

    def partner(value):
        return lax.ppermute(value, "tp", swap)

    def around(value, steps=1):
        return lax.ppermute(
            value, "fs", [(i, (i + 2 * steps) % n_fs) for i in range(n_fs)]
        )

    place = jnp.stack([rep, col, core, ring]).astype(jnp.int32)

    own = jnp.stack([pool_input.astype(BF), pool_output.astype(BF)])
    mine = [lax.dynamic_slice_in_dim(own, rep * half, half, axis=1)]
    mine += [around(mine[0])]
    mine += [around(mine[1], k - 1) for k in range(2, n_ring - 1)]
    mine += [around(mine[0], -1)]
    other = beside(own)
    rest = []
    for k in range(1, n_ring):
        next_to, facing = beside(mine[k]), across(mine[k])
        last = across(next_to)
        rest += [mine[k], facing, next_to, last]

    own_scale = jnp.stack([output_scale, down_scale])
    pair = jnp.stack([own_scale, beside(own_scale)])
    scales = [pair]
    for _ in range(1, n_ring):
        scales.append(around(scales[-1]))

    def circled(start, back):
        chain = [start, around(start)]
        for _ in range(2, n_ring - back):
            chain.append(around(chain[-1]))
        if back:
            chain.append(around(start, -1))
        return [(c, partner(c)) for c in chain]

    kept, kept_late, sent, sent_late, gated_scale = run_pack(
        place, gate_weight, up_weight, gate_scale[None], up_scale[None]
    )
    gated_parts = [
        sum((a + b for a, b in zip(circled(first, 0), circled(beside(second), 0))), ())
        for first, second in ((kept, sent), (kept_late, sent_late))
    ]
    down_kept, down_sent = run_turn(place, down_weight)
    down_parts = circled(jnp.stack([down_kept, beside(down_sent)]), 1)

    tokens, normed, next_gain = run_ready(place, n_ring, tokens, mixer_gain[None], channel_gain[None])
    part_mine, part_away = run_mixer(
        place, normed, input_scale[None], group_mix, group_scale[None], scales, own,
        other, rest,
    )
    middle_mine, here = run_settle(place, tokens, part_mine, partner(part_away), next_gain)

    ax, ay = across(here), beside(here)
    cut = rows // 2
    far = [across(ay[:cut]), beside(ax[cut:])]
    other_scale = partner(gated_scale)
    early, gathered = run_gated(place, gated_scale, other_scale, [here, ax, ay] + far, gated_parts[0], 0)
    late = run_gated(place, gated_scale, other_scale, [gathered], gated_parts[1], kept.shape[1])

    pieces = []
    steps = (0, 1) + tuple(range(n_ring - 1, 1, -1))
    for k in steps:
        base, to_x, to_y, to_far = run_keep(place, early, late, scales[k], middle_mine, down_parts[k], k)
        total = run_join(
            base, across(to_x), beside(to_y),
            corner(to_far),
        )
        pieces.append((total, partner(total)))
    most = run_collect(place, n_ring, steps[:-1], sum(pieces[:-1], ()))
    return run_collect(place, n_ring, steps[-1:], pieces[-1], most)


def solution(mesh):
    in_specs = (
        P(("rep", "fs"), None), P(), P("fs", "tp"), P("tp"), P(None, "tp"), P("tp"), P("fs", "tp"),
        P("fs"), P(), P("fs", "tp"), P("tp"), P("fs", "tp"), P("tp"), P("fs", "tp"), P("fs"),
    )
    out_specs = P(("rep", "fs"), None)
    n_rep, n_fs, n_tp = (mesh.shape[a] for a in ("rep", "fs", "tp"))
    shared = n_rep == 2 and n_tp == 2 and n_fs == 8

    def body(*args):
        return shared_body(n_fs, *args) if shared else plain_body(*args)

    return jax.shard_map(body, mesh=mesh, in_specs=in_specs, out_specs=out_specs, check_vma=False)
```
